32 devices in a mesh: sp: 16 (over z, y, x), tp: 2 (over core).
Axes of the slice: x: 2, y: 2, z: 4, core: 2. Of those that a mesh axis runs over, the one named last changes fastest.
Arguments:
- resid: bfloat16 [2048, 2048], P(('sp', 'tp')), may hold values from -3 to 3
- queries: bfloat16 [2048, 2048], P('sp', 'tp'), may hold values from -6 to 6
- keys: bfloat16 [2048, 2048], P('sp', 'tp'), may hold values from -6 to 6
- values: bfloat16 [2048, 2048], P('sp', 'tp'), may hold values from -8 to 8
- doc_ids: int32 [2048], P('sp'), may hold values from 0 to 3, never falling along the last dimension, each value on 1 to 896 neighbouring positions
- score_offset: float32 [32], P('tp'), may hold values from -10 to -3
- out_weight: bfloat16 [2048, 2048], P('tp'), may hold values from -0.1875 to 0.1875
- norm_gain: float32 [2048], replicated, may hold values from 0.1 to 1.9
- gate_weight: bfloat16 [2048, 6144], P('sp', 'tp'), may hold values from -0.125 to 0.125
- up_weight: bfloat16 [2048, 6144], P('sp', 'tp'), may hold values from -0.125 to 0.125
- down_weight: bfloat16 [6144, 2048], P('tp', 'sp'), may hold values from -0.078125 to 0.078125
Outputs:
- layer_out: bfloat16 [2048, 2048], P(('sp', 'tp'))
The draws below stay inside these ranges and needn't reach their ends.
Inputs may be any that keep to these rules, and one draw needn't show every extreme that they name: `doc_ids`: document numbers never fall along the sequence; each document has 1 to 896 positions, and one has exactly 896.
All inputs are finite; a program needn't handle non-finite values.
Results may differ from the reference program's by a relative error of at most 0.017.
Values may be sent and summed in bfloat16 or wider, within the bound.
A program may use at most 128 MiB of HBM per device.

```python
import math
import jax
import jax.numpy as jnp
import numpy as np
from jax import lax

D = 2048
HEADS = 32
HEAD_DIM = 64
FF = 6144
TOK_DEV = 128
TOKENS = 2048
DOCS = 4
DOC_MOST = 896
N_TP = 2


def draw_score_offset(key, part):
    pick_key = jax.random.fold_in(key, 11)
    slow_key = jax.random.fold_in(key, 12)
    fast_key = jax.random.fold_in(key, 13)
    quick = jax.random.bernoulli(pick_key, 0.5, (HEADS,))
    rate = jax.random.uniform(slow_key, (HEADS,), jnp.float32, 0.5, 2.5)
    slow_offset = jnp.log(rate / DOC_MOST) - 0.5
    fast_offset = jnp.log(jax.random.uniform(fast_key, (HEADS,), jnp.float32, 1.0 / 80.0, 1.0 / 30.0)) - 0.5
    return jnp.clip(jnp.where(quick, fast_offset, slow_offset), -10.0, -3.0).astype(jnp.float32)


def draw_values(key, part):
    span_key = jax.random.fold_in(key, 21)
    noise_key = jax.random.fold_in(key, 22)
    width = HEADS * HEAD_DIM
    spans = TOKENS // TOK_DEV
    common = jax.random.normal(span_key, (spans, 1, width), jnp.float32)
    noise = 0.5 * jax.random.normal(noise_key, (spans, TOK_DEV, width), jnp.float32)
    return jnp.clip(common + noise, -8.0, 8.0).reshape(TOKENS, width).astype(jnp.bfloat16)


def shard_levels(own_key, dims, split, smallest, top_value):
    def one(position, shards_of):
        draws = jax.random.uniform(jax.random.fold_in(jax.random.fold_in(own_key, 6), position), (shards_of,), jnp.float32, smallest / len(split), top_value / len(split))
        return jnp.repeat(jnp.exp(draws), dims[position] // shards_of).reshape((-1,) + (1,) * (len(dims) - position - 1))

    factor_of = one(*split[0])
    for cut in split[1:]:
        factor_of = factor_of * one(*cut)
    return factor_of


def profile(amount, total, reach, slope):
    loads = [(1 << 20) // math.isqrt(grade ** slope) + 1 for grade in range(2, amount + 1)]
    surplus, counts = total - reach - (amount - 1), [1] * (amount - 1)
    while surplus > 0:
        movable = [i for i in range(amount - 1) if counts[i] < reach]
        whole, left = sum([loads[i] for i in movable]), surplus
        for i in movable:
            addition = min(reach - counts[i], max(1, left * loads[i] // whole), surplus)
            counts[i] = counts[i] + addition
            surplus = surplus - addition
    return np.array([reach] + counts)


def uneven_parts(stream_key, number_of, total, bound, skew):
    if number_of == 2:
        one = jax.random.randint(stream_key, (), max(1, total - bound), min(bound, total - 1) + 1)
        return jnp.stack([one, total - one])
    lengths = jnp.asarray(profile(number_of, total, bound, skew), jnp.int32)
    couples = (number_of - 1) // 2
    source_of, taker = lengths[1:1 + 2 * couples:2], lengths[2:2 + 2 * couples:2]
    margin = jnp.minimum(source_of - 1, bound - taker)
    moved = jax.random.randint(jax.random.fold_in(stream_key, 1), (couples,), 0, 1 << 20) % (margin + 1)
    lengths = lengths.at[1:1 + 2 * couples:2].set(source_of - moved).at[2:2 + 2 * couples:2].set(taker + moved)
    return lengths[jax.random.permutation(jax.random.fold_in(stream_key, 2), number_of)]


def gaussian(rng, shape, deviation, most, split=(), held_as=jnp.bfloat16):
    entries = jax.random.normal(rng, shape, jnp.float32) * deviation
    if len(split) > 0:
        entries = shard_levels(rng, shape, split, -0.22, 0.18) * entries
    return jnp.clip(entries, min=-most, max=most).astype(held_as)


def setup_inputs(seed: int = 0) -> dict:
    seeds = jax.random.split(jax.random.key(seed), 12)
    resid = gaussian(seeds[0], (TOKENS, D), 0.5, 3.0, ((0, 32),))
    queries = gaussian(seeds[1], (TOKENS, HEADS * HEAD_DIM), 1.0, 6.0, ((0, 16), (1, 2)))
    keys = gaussian(seeds[2], (TOKENS, HEADS * HEAD_DIM), 1.0, 6.0, ((0, 16), (1, 2)))
    values = draw_values(jax.random.fold_in(seeds[11], 71), 0)
    doc_ids = jnp.searchsorted(jnp.cumsum(uneven_parts(seeds[4], DOCS, TOKENS, DOC_MOST, 1)), jnp.arange(TOKENS), side="right").astype(jnp.int32)
    score_offset = draw_score_offset(jax.random.fold_in(seeds[11], 71), 0)
    out_weight = gaussian(seeds[6], (HEADS * HEAD_DIM, D), (HEADS * HEAD_DIM // 2) ** -0.5, 0.1875, ((0, 2),))
    norm_gain = jnp.clip(1.0 + 0.18 * jax.random.normal(seeds[7], (D,), jnp.float32), 0.1, 1.9)
    gate_weight = gaussian(seeds[8], (D, FF), D ** -0.5, 0.125, ((0, 16), (1, 2)))
    up_weight = gaussian(seeds[9], (D, FF), D ** -0.5, 0.125, ((0, 16), (1, 2)))
    down_weight = gaussian(seeds[10], (FF, D), FF ** -0.5, 0.078125, ((0, 2), (1, 16)))
    return dict(resid=resid, queries=queries, keys=keys, values=values, doc_ids=doc_ids, score_offset=score_offset, out_weight=out_weight, norm_gain=norm_gain, gate_weight=gate_weight, up_weight=up_weight, down_weight=down_weight)


def head_attention(q_head, k_head, v_head, doc_ids, offset):
    q_block = math.gcd(TOKENS, 512)
    extent = min(TOKENS, q_block + DOC_MOST)
    blocks = TOKENS // q_block
    scale = HEAD_DIM ** (-0.5)

    def block(index):
        start = (index * q_block).astype(jnp.int32)
        k_start = jnp.clip(start + q_block - extent, 0, TOKENS - extent).astype(jnp.int32)
        q_rows = lax.dynamic_slice_in_dim(q_head, start, q_block, 0)
        q_docs = lax.dynamic_slice_in_dim(doc_ids, start, q_block, 0)
        k_rows = lax.dynamic_slice_in_dim(k_head, k_start, extent, 0)
        v_rows = lax.dynamic_slice_in_dim(v_head, k_start, extent, 0)
        k_docs = lax.dynamic_slice_in_dim(doc_ids, k_start, extent, 0)
        q_pos = start + jnp.arange(q_block, dtype=jnp.int32)
        key_pos = k_start + jnp.arange(extent, dtype=jnp.int32)
        scores = lax.dot_general(q_rows, k_rows, (((1,), (1,)), ((), ())), preferred_element_type=jnp.float32) * scale + offset
        live = (key_pos[None, :] < q_pos[:, None]) & (k_docs[None, :] == q_docs[:, None])
        log_keep = jnp.where(live, jax.nn.log_sigmoid(-scores), 0.0)
        tail = lax.cumsum(log_keep, axis=1, reverse=True) - log_keep
        weight = jnp.where(live, jnp.exp(jax.nn.log_sigmoid(scores) + tail), 0.0).astype(jnp.bfloat16)
        return jnp.dot(weight, v_rows, preferred_element_type=jnp.float32).astype(jnp.bfloat16)
    result = lax.map(block, jnp.arange(blocks, dtype=jnp.int32))
    return result.reshape(TOKENS, HEAD_DIM)

def reference(resid, queries, keys, values, doc_ids, score_offset, out_weight, norm_gain, gate_weight, up_weight, down_weight):
    heads_out = []
    for head in range(HEADS):
        cols = slice(head * HEAD_DIM, (head + 1) * HEAD_DIM)
        heads_out.append(head_attention(queries[:, cols], keys[:, cols], values[:, cols], doc_ids, score_offset[head]))
    attended = jnp.concatenate(heads_out, axis=1)
    group_width = HEADS // N_TP * HEAD_DIM
    mixed_attn = jnp.zeros((TOKENS, D), jnp.float32)
    for group in range(N_TP):
        cols = slice(group * group_width, (group + 1) * group_width)
        partial_out = jnp.dot(attended[:, cols], out_weight[cols, :], preferred_element_type=jnp.float32)
        mixed_attn = mixed_attn + partial_out.astype(jnp.bfloat16).astype(jnp.float32)
    stream = resid.astype(jnp.float32) + mixed_attn
    normed = (stream * lax.rsqrt(lax.optimization_barrier(jnp.mean(stream * stream, axis=1, keepdims=True)) + 1e-06) * norm_gain).astype(jnp.bfloat16)
    unit_width = FF // N_TP
    feed = jnp.zeros((TOKENS, D), jnp.float32)
    for group in range(N_TP):
        cols = slice(group * unit_width, (group + 1) * unit_width)
        gate = jnp.dot(normed, gate_weight[:, cols], preferred_element_type=jnp.float32)
        upper = jnp.dot(normed, up_weight[:, cols], preferred_element_type=jnp.float32)
        hidden = (jax.nn.silu(gate) * upper).astype(jnp.bfloat16)
        partial_out = jnp.dot(hidden, down_weight[cols, :], preferred_element_type=jnp.float32)
        feed = feed + partial_out.astype(jnp.bfloat16).astype(jnp.float32)
    return (stream + feed).astype(jnp.bfloat16)
```

```python
import functools

import jax
import jax.numpy as jnp
from jax import lax
from jax.experimental import pallas as pl
from jax.experimental.pallas import tpu as pltpu
from jax.sharding import PartitionSpec as P


def from_behind(shard, axis, by):
    peers = lax.axis_size(axis)
    pairs = [(i, i + by) for i in range(peers) if 0 <= i + by < peers]
    return lax.ppermute(shard, axis, pairs)


def as_sent(shard):
    return jax.tree.map(lambda a: a.astype(jnp.bfloat16) if a.dtype == jnp.float32 else a, shard)


def joined(earlier, later):
    return (
        jnp.concatenate([earlier[0], later[0]], axis=0),
        jnp.concatenate([earlier[1], later[1]], axis=0),
        jnp.concatenate([earlier[2], later[2]], axis=0),
    )


def block_update(carry, block, start, context):
    queries_h, q_pos, q_docs, offsets, scale = context
    total, carried = carry
    k_block, v_block, d_block = block
    count = k_block.shape[0]
    heads = offsets.shape[0]
    head_dim = queries_h.shape[2]

    def compute():
        key_pos = start + jnp.arange(count, dtype=jnp.int32)
        live = (
            (key_pos[None, :] >= 0)
            & (key_pos[None, :] < q_pos[:, None])
            & (d_block[None, :] == q_docs[:, None])
        )
        k_heads = k_block.reshape(count, heads, head_dim)
        v_heads = v_block.reshape(count, heads, head_dim)
        scores = (
            jnp.einsum("thd,shd->hts", queries_h, k_heads, preferred_element_type=jnp.float32)
            * scale
            + offsets[:, None, None]
        )
        log_keep = jnp.where(live[None], jax.nn.log_sigmoid(-scores), 0.0)
        tail = lax.cumsum(log_keep, axis=2, reverse=True) - log_keep + carried[:, :, None]
        weight = jnp.where(live[None], jnp.exp(jax.nn.log_sigmoid(scores) + tail), 0.0).astype(
            jnp.bfloat16
        )
        added = jnp.einsum("hts,shd->thd", weight, v_heads, preferred_element_type=jnp.float32)
        return (total + added, carried + jnp.sum(log_keep, axis=2))

    reached = (start + count > 0) & (d_block[-1] >= q_docs[0])
    return lax.cond(reached, compute, lambda: carry)


def windowed(
    resid,
    queries,
    keys,
    values,
    doc_ids,
    score_offset,
    out_weight,
    norm_gain,
    gate_weight,
    up_weight,
    down_weight,
):
    rows = queries.shape[0]
    heads = score_offset.shape[0]
    head_dim = queries.shape[1] // heads
    base = lax.axis_index("sp") * rows
    q_pos = base + jnp.arange(rows, dtype=jnp.int32)
    context = (
        queries.reshape(rows, heads, head_dim),
        q_pos,
        doc_ids,
        score_offset,
        head_dim ** (-0.5),
    )
    own = (keys, values, doc_ids)
    carry = (jnp.zeros((rows, heads, head_dim), jnp.float32), jnp.zeros((heads, rows), jnp.float32))
    nearest = from_behind((keys, values, doc_ids), "sp", 1)
    paired = joined(nearest, own)
    carry = block_update(carry, paired, base - rows, context)
    middle = from_behind((paired[0], paired[1], as_sent(paired[2])), "sp", 2)
    carry = block_update(carry, middle, base - 3 * rows, context)
    fourfold = joined(middle, paired)
    farthest = from_behind((fourfold[0], fourfold[1], as_sent(fourfold[2])), "sp", 4)
    carry = block_update(
        carry, tuple((piece[2 * rows :] for piece in farthest)), base - 5 * rows, context
    )
    carry = block_update(
        carry, tuple((piece[: 2 * rows] for piece in farthest)), base - 7 * rows, context
    )
    attended = carry[0].reshape(rows, heads * head_dim).astype(jnp.bfloat16)
    mixed_attn = lax.psum_scatter(
        jnp.dot(attended, out_weight, preferred_element_type=jnp.float32).astype(jnp.bfloat16),
        "tp",
        scatter_dimension=0,
        tiled=True,
    ).astype(jnp.float32)
    stream = resid.astype(jnp.float32) + mixed_attn
    normed = (
        stream * lax.rsqrt(jnp.mean(stream * stream, axis=1, keepdims=True) + 1e-06) * norm_gain
    ).astype(jnp.bfloat16)
    span_rows = lax.all_gather(normed, "tp", axis=0, tiled=True)
    gate = jnp.dot(
        span_rows,
        lax.all_gather(gate_weight, "sp", axis=0, tiled=True),
        preferred_element_type=jnp.float32,
    )
    upper = jnp.dot(
        span_rows,
        lax.all_gather(up_weight, "sp", axis=0, tiled=True),
        preferred_element_type=jnp.float32,
    )
    hidden = (jax.nn.silu(gate) * upper).astype(jnp.bfloat16)
    partial_out = jnp.dot(
        hidden,
        lax.all_gather(down_weight, "sp", axis=1, tiled=True),
        preferred_element_type=jnp.float32,
    )
    feed = lax.psum_scatter(
        partial_out.astype(jnp.bfloat16), "tp", scatter_dimension=0, tiled=True
    ).astype(jnp.float32)
    return (stream + feed).astype(jnp.bfloat16)


DOC_MOST = 896
MESH = pl.DeviceIdType.MESH


def sends(src, dst, send, recv, target):
    return pltpu.make_async_remote_copy(
        src_ref=src, dst_ref=dst, send_sem=send, recv_sem=recv, device_id=target, device_id_type=MESH
    )


def head_kernel(
    n,
    q_ref, k_ref, v_ref, doc_ref, off_ref, g_in, u_in, d_in,
    att_ref, wg, wu, wd,
    sbuf, rbuf, docr, ao,
    qkv_s, qkv_r, doc_s, doc_r, att_s, att_r, w_s, w_r, f_s, own_sem,
):
    s = lax.axis_index("sp")
    c = lax.axis_index("tp")
    rows = q_ref.shape[0]
    half = rows // 2
    dim = q_ref.shape[1] // n
    ntp = wg.shape[1] * n // g_in.shape[1]
    per = n // ntp
    width = wg.shape[1]
    depth = g_in.shape[0]
    dcols = d_in.shape[1]
    back = -(-DOC_MOST // rows)
    other = 1 - c

    for j in range(n // 2):
        cols = slice(j * 2 * dim, (j + 1) * 2 * dim)
        kp, vp, qp = (r[:, cols].astype(jnp.float32) for r in (k_ref, v_ref, q_ref))
        low = lax.broadcasted_iota(jnp.int32, (rows, 2 * dim), 1) < dim
        lowh = low[:half]
        top, bot = qp[:half], qp[half:]
        sbuf[2 * j, :rows, :] = jnp.where(low, kp, pltpu.roll(vp, dim, 1)).astype(jnp.bfloat16)
        sbuf[2 * j + 1, :rows, :] = jnp.where(low, pltpu.roll(kp, dim, 1), vp).astype(jnp.bfloat16)
        sbuf[2 * j, rows:, :] = jnp.where(lowh, top, pltpu.roll(bot, dim, 1)).astype(jnp.bfloat16)
        sbuf[2 * j + 1, rows:, :] = jnp.where(lowh, pltpu.roll(top, dim, 1), bot).astype(jnp.bfloat16)

    def qkv_copy(t, src):
        return sends(sbuf.at[t], rbuf.at[src], qkv_s.at[t], qkv_r.at[src], {"sp": t})

    def doc_copy(t, src):
        return sends(doc_ref, docr.at[src], doc_s.at[t], doc_r.at[src], {"sp": t})

    def start_peer(k, _):
        t = lax.rem(s + k, n)
        qkv_copy(t, s).start()
        doc_copy(t, s).start()
        return 0

    lax.fori_loop(1, n, start_peer, 0)
    rbuf[pl.ds(s, 1)] = sbuf[pl.ds(s, 1)]
    docr[pl.ds(s, 1)] = doc_ref[...][None]

    tc = lax.rem(s, 2)
    mats = ((g_in, wg), (u_in, wu), (d_in, wd))

    def part_of(m, p):
        start = pl.multiple_of((p - per * c) * width, width)
        return mats[m][0].at[pl.ds(start, width), :] if m == 2 else mats[m][0].at[:, pl.ds(start, width)]

    def slot_of(m, src):
        if m == 2:
            return mats[m][1].at[:, pl.ds(pl.multiple_of(src * dcols, dcols), dcols)]
        return mats[m][1].at[pl.ds(pl.multiple_of(src * depth, depth), depth), :]

    def w_copy(m, p, k):
        return sends(part_of(m, p), slot_of(m, s), w_s.at[m, k], w_r.at[m, s], {"sp": p, "tp": tc})

    def own_copy(m, p):
        return pltpu.make_async_copy(part_of(m, p), slot_of(m, s), own_sem.at[m])

    for m in range(3):

        def start_weight(k, _, m=m):
            p = per * c + lax.rem(s + k, per)
            mine = (p == s) & (tc == c)

            @pl.when(mine)
            def _():
                own_copy(m, p).start()

            @pl.when(jnp.logical_not(mine))
            def _():
                w_copy(m, p, k).start()

            return 0

        lax.fori_loop(0, per, start_weight, 0)

    def wait_peer(k, _):
        src = lax.rem(s + n - k, n)
        qkv_copy(src, src).wait_recv()
        doc_copy(src, src).wait_recv()
        return 0

    lax.fori_loop(1, n, wait_peer, 0)

    scale = dim ** (-0.5)
    off = off_ref[s]
    lane = lax.broadcasted_iota(jnp.int32, (half, 2 * dim), 1) < dim
    row_i = lax.broadcasted_iota(jnp.int32, (rows, rows), 0)
    col_i = lax.broadcasted_iota(jnp.int32, (rows, rows), 1)
    later = (row_i > col_i).astype(jnp.bfloat16)
    nt = (((1,), (1,)), ((), ()))

    def att_copy(t, src):
        return sends(ao.at[t], att_ref.at[src], att_s.at[t], att_r.at[src], {"sp": t})

    def block(step, _):
        i = lax.rem(s + step, n)
        q2 = rbuf[i, rows:, :].astype(jnp.float32)
        q_pad = jnp.concatenate(
            [jnp.where(lane, q2, 0.0), jnp.where(lane, pltpu.roll(q2, dim, 1), 0.0)], axis=0
        ).astype(jnp.bfloat16)
        q_doc = jnp.broadcast_to(docr[i, 0:1, :].astype(jnp.float32), (rows, rows)).T
        total = jnp.zeros((rows, 2 * dim), jnp.float32)
        carried = jnp.zeros((rows, 1), jnp.float32)
        for d in range(min(back, n - 1) + 1):
            j = jnp.maximum(i - d, 0)
            kv = rbuf[j, :rows, :]
            k_doc = jnp.where(i >= d, docr[j, 0:1, :].astype(jnp.float32), -1.0)
            z = lax.dot_general(q_pad, kv, nt, preferred_element_type=jnp.float32) * scale + off
            live = q_doc == k_doc
            if d == 0:
                live = live & (col_i < row_i)
            soft = jnp.log(1.0 + jnp.exp(-jnp.abs(z)))
            keep = jnp.where(live, -jnp.maximum(z, 0.0) - soft, 0.0)
            high = keep.astype(jnp.bfloat16)
            rest = (keep - high.astype(jnp.float32)).astype(jnp.bfloat16)
            tail = jnp.dot(high, later, preferred_element_type=jnp.float32) + jnp.dot(
                rest, later, preferred_element_type=jnp.float32
            )
            weight = jnp.where(
                live, jnp.exp(jnp.minimum(z, 0.0) - soft + (tail + carried)), 0.0
            ).astype(jnp.bfloat16)
            total = total + jnp.dot(weight, kv, preferred_element_type=jnp.float32)
            carried = carried + jnp.sum(keep, axis=1, keepdims=True)
        packed = jnp.where(lane, pltpu.roll(total[:half], dim, 1), total[half:]).astype(jnp.bfloat16)

        @pl.when(i == s)
        def _():
            att_ref[pl.ds(s, 1)] = packed[None]

        @pl.when(i != s)
        def _():
            ao[pl.ds(i, 1)] = packed[None]
            att_copy(i, s).start()

        return 0

    lax.fori_loop(0, n, block, 0)

    def forward(m, src, k):
        return sends(slot_of(m, src), slot_of(m, src), f_s.at[m, k], w_r.at[m, src], {"tp": other})

    base_c = s // per
    for m in range(3):

        def pass_on(k, _, m=m):
            src = 2 * k + c
            mine = (src == s) & (base_c == c)

            @pl.when(mine)
            def _():
                own_copy(m, s).wait()

            @pl.when(jnp.logical_not(mine))
            def _():
                forward(m, src, k).wait_recv()

            forward(m, src, k).start()
            return 0

        lax.fori_loop(0, n // 2, pass_on, 0)

    def finish_peer(k, _):
        src = lax.rem(s + n - k, n)
        att_copy(src, src).wait_recv()
        att_copy(src, src).wait_send()
        qkv_copy(src, src).wait_send()
        doc_copy(src, src).wait_send()
        return 0

    lax.fori_loop(1, n, finish_peer, 0)
    for m in range(3):

        def finish_forward(k, _, m=m):
            forward(m, 2 * k + other, k).wait_recv()
            forward(m, 2 * k + c, k).wait_send()
            return 0

        lax.fori_loop(0, n // 2, finish_forward, 0)

        def finish_weight(k, _, m=m):
            p = per * c + lax.rem(s + k, per)

            @pl.when(jnp.logical_not((p == s) & (tc == c)))
            def _():
                w_copy(m, p, k).wait_send()

            return 0

        lax.fori_loop(0, per, finish_weight, 0)


def heads_and_weights(n, ntp, queries, keys, values, doc_ids, score_offset, gate_weight, up_weight, down_weight):
    rows, local = queries.shape
    half, two = rows // 2, 2 * (local // n)
    d_model = n * gate_weight.shape[0]
    width = gate_weight.shape[1] * ntp // n
    bf = jnp.bfloat16
    vmem = pl.BlockSpec(memory_space=pltpu.VMEM)
    anyw = pl.BlockSpec(memory_space=pl.ANY)
    dma = pltpu.SemaphoreType.DMA
    per = n // ntp
    return pl.pallas_call(
        functools.partial(head_kernel, n),
        out_shape=(
            jax.ShapeDtypeStruct((n, half, two), bf),
            jax.ShapeDtypeStruct((d_model, width), bf),
            jax.ShapeDtypeStruct((d_model, width), bf),
            jax.ShapeDtypeStruct((width, d_model), bf),
        ),
        in_specs=[vmem] * 4 + [pl.BlockSpec(memory_space=pltpu.SMEM)] + [anyw] * 3,
        out_specs=(vmem, anyw, anyw, anyw),
        scratch_shapes=[
            pltpu.VMEM((n, rows + half, two), bf),
            pltpu.VMEM((n, rows + half, two), bf),
            pltpu.VMEM((n, 8, rows), jnp.int32),
            pltpu.VMEM((n, half, two), bf),
            dma((n,)), dma((n,)), dma((n,)), dma((n,)), dma((n,)), dma((n,)),
            dma((3, per)), dma((3, n)), dma((3, n // 2)), dma((3,)),
        ],
        compiler_params=pltpu.CompilerParams(has_side_effects=True, vmem_limit_bytes=48 << 20),
    )(
        queries, keys, values, jnp.broadcast_to(doc_ids[None], (8, rows)), score_offset,
        gate_weight, up_weight, down_weight,
    )


def resharded(
    resid, queries, keys, values, doc_ids, score_offset, out_weight, norm_gain,
    gate_weight, up_weight, down_weight,
):
    n, ntp = lax.axis_size("sp"), lax.axis_size("tp")
    rows, local = queries.shape
    half, dim = rows // 2, local // n
    att, wg, wu, wd = heads_and_weights(
        n, ntp, queries, keys, values, doc_ids, score_offset, gate_weight, up_weight, down_weight
    )
    attended = att.reshape(n, half, 2, dim).transpose(2, 1, 0, 3).reshape(rows, local)
    mixed_attn = lax.psum_scatter(
        jnp.dot(attended, out_weight, preferred_element_type=jnp.float32).astype(jnp.bfloat16),
        "tp", scatter_dimension=0, tiled=True,
    ).astype(jnp.float32)
    stream = resid.astype(jnp.float32) + mixed_attn
    normed = (
        stream * lax.rsqrt(jnp.mean(stream * stream, axis=1, keepdims=True) + 1e-06) * norm_gain
    ).astype(jnp.bfloat16)
    every = lax.all_gather(normed, "sp", axis=0, tiled=True)
    gate = jnp.dot(every, wg, preferred_element_type=jnp.float32)
    upper = jnp.dot(every, wu, preferred_element_type=jnp.float32)
    hidden = (jax.nn.silu(gate) * upper).astype(jnp.bfloat16)
    partial_out = jnp.dot(hidden, wd, preferred_element_type=jnp.float32).astype(jnp.bfloat16)
    feed = lax.psum_scatter(partial_out, "sp", scatter_dimension=0, tiled=True)
    return (stream + feed.astype(jnp.float32)).astype(jnp.bfloat16)


def on_device(*args):
    queries, doc_ids, score_offset, gate_weight = args[1], args[4], args[5], args[8]
    n, ntp = lax.axis_size("sp"), lax.axis_size("tp")
    dim = queries.shape[1] // score_offset.shape[0]
    fits = (
        ntp == 2
        and score_offset.shape[0] == n
        and 2 * dim == 128
        and doc_ids.shape[0] == 128
        and n % 2 == 0
        and gate_weight.shape[1] * ntp % (n * 128) == 0
        and gate_weight.shape[0] % 128 == 0
    )
    return resharded(*args) if fits else windowed(*args)


def solution(mesh):
    in_specs = (
        P(("sp", "tp"), None),
        P("sp", "tp"),
        P("sp", "tp"),
        P("sp", "tp"),
        P("sp"),
        P("tp"),
        P("tp", None),
        P(),
        P("sp", "tp"),
        P("sp", "tp"),
        P("tp", "sp"),
    )
    out_specs = P(("sp", "tp"), None)
    return jax.shard_map(
        on_device, mesh=mesh, in_specs=in_specs, out_specs=out_specs, check_vma=False
    )
```

```python
import functools

import jax
import jax.numpy as jnp
from jax import lax
from jax.experimental import pallas as pl
from jax.experimental.pallas import tpu as pltpu
from jax.sharding import PartitionSpec as P


def from_behind(shard, axis, by):
    peers = lax.axis_size(axis)
    pairs = [(i, i + by) for i in range(peers) if 0 <= i + by < peers]
    return lax.ppermute(shard, axis, pairs)


def as_sent(shard):
    return jax.tree.map(lambda a: a.astype(jnp.bfloat16) if a.dtype == jnp.float32 else a, shard)


def joined(earlier, later):
    return (
        jnp.concatenate([earlier[0], later[0]], axis=0),
        jnp.concatenate([earlier[1], later[1]], axis=0),
        jnp.concatenate([earlier[2], later[2]], axis=0),
    )


def block_update(carry, block, start, context):
    queries_h, q_pos, q_docs, offsets, scale = context
    total, carried = carry
    k_block, v_block, d_block = block
    count = k_block.shape[0]
    heads = offsets.shape[0]
    head_dim = queries_h.shape[2]

    def compute():
        key_pos = start + jnp.arange(count, dtype=jnp.int32)
        live = (
            (key_pos[None, :] >= 0)
            & (key_pos[None, :] < q_pos[:, None])
            & (d_block[None, :] == q_docs[:, None])
        )
        k_heads = k_block.reshape(count, heads, head_dim)
        v_heads = v_block.reshape(count, heads, head_dim)
        scores = (
            jnp.einsum("thd,shd->hts", queries_h, k_heads, preferred_element_type=jnp.float32)
            * scale
            + offsets[:, None, None]
        )
        log_keep = jnp.where(live[None], jax.nn.log_sigmoid(-scores), 0.0)
        tail = lax.cumsum(log_keep, axis=2, reverse=True) - log_keep + carried[:, :, None]
        weight = jnp.where(live[None], jnp.exp(jax.nn.log_sigmoid(scores) + tail), 0.0).astype(
            jnp.bfloat16
        )
        added = jnp.einsum("hts,shd->thd", weight, v_heads, preferred_element_type=jnp.float32)
        return (total + added, carried + jnp.sum(log_keep, axis=2))

    reached = (start + count > 0) & (d_block[-1] >= q_docs[0])
    return lax.cond(reached, compute, lambda: carry)


def windowed(
    resid,
    queries,
    keys,
    values,
    doc_ids,
    score_offset,
    out_weight,
    norm_gain,
    gate_weight,
    up_weight,
    down_weight,
):
    rows = queries.shape[0]
    heads = score_offset.shape[0]
    head_dim = queries.shape[1] // heads
    base = lax.axis_index("sp") * rows
    q_pos = base + jnp.arange(rows, dtype=jnp.int32)
    context = (
        queries.reshape(rows, heads, head_dim),
        q_pos,
        doc_ids,
        score_offset,
        head_dim ** (-0.5),
    )
    own = (keys, values, doc_ids)
    carry = (jnp.zeros((rows, heads, head_dim), jnp.float32), jnp.zeros((heads, rows), jnp.float32))
    nearest = from_behind((keys, values, doc_ids), "sp", 1)
    paired = joined(nearest, own)
    carry = block_update(carry, paired, base - rows, context)
    middle = from_behind((paired[0], paired[1], as_sent(paired[2])), "sp", 2)
    carry = block_update(carry, middle, base - 3 * rows, context)
    fourfold = joined(middle, paired)
    farthest = from_behind((fourfold[0], fourfold[1], as_sent(fourfold[2])), "sp", 4)
    carry = block_update(
        carry, tuple((piece[2 * rows :] for piece in farthest)), base - 5 * rows, context
    )
    carry = block_update(
        carry, tuple((piece[: 2 * rows] for piece in farthest)), base - 7 * rows, context
    )
    attended = carry[0].reshape(rows, heads * head_dim).astype(jnp.bfloat16)
    mixed_attn = lax.psum_scatter(
        jnp.dot(attended, out_weight, preferred_element_type=jnp.float32).astype(jnp.bfloat16),
        "tp",
        scatter_dimension=0,
        tiled=True,
    ).astype(jnp.float32)
    stream = resid.astype(jnp.float32) + mixed_attn
    normed = (
        stream * lax.rsqrt(jnp.mean(stream * stream, axis=1, keepdims=True) + 1e-06) * norm_gain
    ).astype(jnp.bfloat16)
    span_rows = lax.all_gather(normed, "tp", axis=0, tiled=True)
    gate = jnp.dot(
        span_rows,
        lax.all_gather(gate_weight, "sp", axis=0, tiled=True),
        preferred_element_type=jnp.float32,
    )
    upper = jnp.dot(
        span_rows,
        lax.all_gather(up_weight, "sp", axis=0, tiled=True),
        preferred_element_type=jnp.float32,
    )
    hidden = (jax.nn.silu(gate) * upper).astype(jnp.bfloat16)
    partial_out = jnp.dot(
        hidden,
        lax.all_gather(down_weight, "sp", axis=1, tiled=True),
        preferred_element_type=jnp.float32,
    )
    feed = lax.psum_scatter(
        partial_out.astype(jnp.bfloat16), "tp", scatter_dimension=0, tiled=True
    ).astype(jnp.float32)
    return (stream + feed).astype(jnp.bfloat16)


DOC_MOST = 896
MESH = pl.DeviceIdType.MESH


def sends(src, dst, send, recv, target):
    return pltpu.make_async_remote_copy(
        src_ref=src, dst_ref=dst, send_sem=send, recv_sem=recv, device_id=target, device_id_type=MESH
    )


def layer_kernel(
    n,
    q_ref, k_ref, v_ref, doc_ref, off_ref, g_in, u_in, d_in, resid_ref, gain_ref, o_in,
    out_ref,
    sbuf, rbuf, docr, ao, att_ref, wg, wu, wd, ow,
    attd, mixed, mixed_in, stream, ag, part, xd, yd, fx, fy, zr,
    qkv_s, qkv_r, doc_s, doc_r, att_s, att_r, w_s, w_r, f_s, own_sem, o_sem, mix_s, mix_r, net_s, net_r,
):
    s = lax.axis_index("sp")
    c = lax.axis_index("tp")
    rows = q_ref.shape[0]
    half = rows // 2
    dim = q_ref.shape[1] // n
    ntp = wg.shape[1] * n // g_in.shape[1]
    per = n // ntp
    width = wg.shape[1]
    depth = g_in.shape[0]
    dcols = d_in.shape[1]
    back = -(-DOC_MOST // rows)
    other = 1 - c
    pltpu.make_async_copy(o_in, ow, o_sem).start()

    for j in range(n // 2):
        cols = slice(j * 2 * dim, (j + 1) * 2 * dim)
        kp, vp, qp = (r[:, cols].astype(jnp.float32) for r in (k_ref, v_ref, q_ref))
        low = lax.broadcasted_iota(jnp.int32, (rows, 2 * dim), 1) < dim
        lowh = low[:half]
        top, bot = qp[:half], qp[half:]
        sbuf[2 * j, :rows, :] = jnp.where(low, kp, pltpu.roll(vp, dim, 1)).astype(jnp.bfloat16)
        sbuf[2 * j + 1, :rows, :] = jnp.where(low, pltpu.roll(kp, dim, 1), vp).astype(jnp.bfloat16)
        sbuf[2 * j, rows:, :] = jnp.where(lowh, top, pltpu.roll(bot, dim, 1)).astype(jnp.bfloat16)
        sbuf[2 * j + 1, rows:, :] = jnp.where(lowh, pltpu.roll(top, dim, 1), bot).astype(jnp.bfloat16)

    def qkv_copy(t, src):
        return sends(sbuf.at[t], rbuf.at[src], qkv_s.at[t], qkv_r.at[src], {"sp": t})

    def doc_copy(t, src):
        return sends(doc_ref, docr.at[src], doc_s.at[t], doc_r.at[src], {"sp": t})

    def start_peer(k, _):
        t = lax.rem(s + k, n)
        qkv_copy(t, s).start()
        doc_copy(t, s).start()
        return 0

    lax.fori_loop(1, n, start_peer, 0)
    rbuf[pl.ds(s, 1)] = sbuf[pl.ds(s, 1)]
    docr[pl.ds(s, 1)] = doc_ref[...][None]

    tc = lax.rem(s, 2)
    mats = ((g_in, wg), (u_in, wu), (d_in, wd))

    def part_of(m, p):
        start = pl.multiple_of((p - per * c) * width, width)
        return mats[m][0].at[pl.ds(start, width), :] if m == 2 else mats[m][0].at[:, pl.ds(start, width)]

    def slot_of(m, src):
        if m == 2:
            return mats[m][1].at[:, pl.ds(pl.multiple_of(src * dcols, dcols), dcols)]
        return mats[m][1].at[pl.ds(pl.multiple_of(src * depth, depth), depth), :]

    def w_copy(m, p, k):
        return sends(part_of(m, p), slot_of(m, s), w_s.at[m, k], w_r.at[m, s], {"sp": p, "tp": tc})

    def own_copy(m, p):
        return pltpu.make_async_copy(part_of(m, p), slot_of(m, s), own_sem.at[m])

    for m in range(3):

        def start_weight(k, _, m=m):
            p = per * c + lax.rem(s + k, per)
            mine = (p == s) & (tc == c)

            @pl.when(mine)
            def _():
                own_copy(m, p).start()

            @pl.when(jnp.logical_not(mine))
            def _():
                w_copy(m, p, k).start()

            return 0

        lax.fori_loop(0, per, start_weight, 0)

    def wait_peer(k, _):
        src = lax.rem(s + n - k, n)
        qkv_copy(src, src).wait_recv()
        doc_copy(src, src).wait_recv()
        return 0

    lax.fori_loop(1, n, wait_peer, 0)

    scale = dim ** (-0.5)
    off = off_ref[s]
    lane = lax.broadcasted_iota(jnp.int32, (half, 2 * dim), 1) < dim
    row_i = lax.broadcasted_iota(jnp.int32, (rows, rows), 0)
    col_i = lax.broadcasted_iota(jnp.int32, (rows, rows), 1)
    later = (row_i > col_i).astype(jnp.bfloat16)
    nt = (((1,), (1,)), ((), ()))

    def att_copy(t, src):
        return sends(ao.at[t], att_ref.at[src], att_s.at[t], att_r.at[src], {"sp": t})

    def block(step, _):
        i = lax.rem(s + step, n)
        q2 = rbuf[i, rows:, :].astype(jnp.float32)
        q_pad = jnp.concatenate(
            [jnp.where(lane, q2, 0.0), jnp.where(lane, pltpu.roll(q2, dim, 1), 0.0)], axis=0
        ).astype(jnp.bfloat16)
        q_doc = jnp.broadcast_to(docr[i, 0:1, :].astype(jnp.float32), (rows, rows)).T
        total = jnp.zeros((rows, 2 * dim), jnp.float32)
        carried = jnp.zeros((rows, 1), jnp.float32)
        for d in range(min(back, n - 1) + 1):
            j = jnp.maximum(i - d, 0)
            kv = rbuf[j, :rows, :]
            k_doc = jnp.where(i >= d, docr[j, 0:1, :].astype(jnp.float32), -1.0)
            z = lax.dot_general(q_pad, kv, nt, preferred_element_type=jnp.float32) * scale + off
            live = q_doc == k_doc
            if d == 0:
                live = live & (col_i < row_i)
            soft = jnp.log(1.0 + jnp.exp(-jnp.abs(z)))
            keep = jnp.where(live, -jnp.maximum(z, 0.0) - soft, 0.0)
            high = keep.astype(jnp.bfloat16)
            rest = (keep - high.astype(jnp.float32)).astype(jnp.bfloat16)
            tail = jnp.dot(high, later, preferred_element_type=jnp.float32) + jnp.dot(
                rest, later, preferred_element_type=jnp.float32
            )
            weight = jnp.where(
                live, jnp.exp(jnp.minimum(z, 0.0) - soft + (tail + carried)), 0.0
            ).astype(jnp.bfloat16)
            total = total + jnp.dot(weight, kv, preferred_element_type=jnp.float32)
            carried = carried + jnp.sum(keep, axis=1, keepdims=True)
        packed = jnp.where(lane, pltpu.roll(total[:half], dim, 1), total[half:]).astype(jnp.bfloat16)

        @pl.when(i == s)
        def _():
            att_ref[pl.ds(s, 1)] = packed[None]

        @pl.when(i != s)
        def _():
            ao[pl.ds(i, 1)] = packed[None]
            att_copy(i, s).start()

        return 0

    lax.fori_loop(0, n, block, 0)

    def wait_attended(k, _):
        src = lax.rem(s + n - k, n)
        att_copy(src, src).wait_recv()
        return 0

    lax.fori_loop(1, n, wait_attended, 0)
    for j in range(n // 2):
        cols = slice(j * 2 * dim, (j + 1) * 2 * dim)
        ha, hb = (att_ref[2 * j + e].astype(jnp.float32) for e in range(2))
        attd[:half, cols] = jnp.where(lane, ha, pltpu.roll(hb, dim, 1)).astype(jnp.bfloat16)
        attd[half:, cols] = jnp.where(lane, pltpu.roll(ha, dim, 1), hb).astype(jnp.bfloat16)

    pltpu.make_async_copy(o_in, ow, o_sem).wait()
    dm = ow.shape[1]
    tile = min(512, dm)

    def project(t, _):
        cols = pl.ds(pl.multiple_of(t * tile, tile), tile)
        prod = jnp.dot(attd[...], ow[:, cols], preferred_element_type=jnp.float32).astype(jnp.bfloat16)
        mixed[0, :, cols] = prod[:half]
        mixed[1, :, cols] = prod[half:]
        return 0

    lax.fori_loop(0, dm // tile, project, 0)
    mix = sends(mixed.at[other], mixed_in, mix_s, mix_r, {"tp": other})
    mix.start()
    mix.wait_recv()
    rows_f = resid_ref[...].astype(jnp.float32) + (
        mixed[c].astype(jnp.float32) + mixed_in[...].astype(jnp.float32)
    )
    stream[...] = rows_f
    inv = lax.rsqrt(jnp.mean(rows_f * rows_f, axis=1, keepdims=True) + 1e-06)
    ag[pl.ds(s, 1)] = (rows_f * inv * gain_ref[...]).astype(jnp.bfloat16)[None]

    levels = n // 4
    quarter = half // 2
    up, down = slice(0, quarter), slice(quarter, half)

    def flip(v, mask):
        bit = 1
        moved = v
        while bit <= mask:
            if mask & bit:
                moved = moved + bit - 2 * bit * lax.rem(lax.div(v, bit), 2)
            bit *= 2
        return moved

    xn, yn = flip(s, 1), flip(s, 2)

    def link(kind, k, src, dst, to):
        return sends(src, dst, net_s.at[kind, k], net_r.at[kind, k], {"sp": to})

    def ids(k):
        return tuple(flip(s, 4 * k + e) for e in range(4))

    def ag_z(k):
        return link(0, k, ag.at[s], ag.at[s], ids(k)[0])

    def ag_x(k):
        return link(1, k, ag.at[ids(k)[0]], ag.at[ids(k)[0]], xn)

    def ag_y(k):
        return link(2, k, ag.at[ids(k)[0]], ag.at[ids(k)[0]], yn)

    def ag_hx(k):
        return link(3, k, ag.at[ids(k)[1], up], ag.at[ids(k)[1], up], yn)

    def ag_hy(k):
        return link(4, k, ag.at[ids(k)[2], down], ag.at[ids(k)[2], down], xn)

    def rs_d1(k):
        return link(5, k, part.at[ids(k)[3], up], xd.at[k], xn)

    def rs_d2(k):
        return link(6, k, part.at[ids(k)[3], down], yd.at[k], yn)

    def rs_px(k):
        return link(7, k, part.at[ids(k)[1], up], fx.at[k, up], xn)

    def rs_qx(k):
        return link(8, k, part.at[ids(k)[1], down], fx.at[k, down], xn)

    def rs_py(k):
        return link(9, k, part.at[ids(k)[2], down], fy.at[k, down], yn)

    def rs_qy(k):
        return link(10, k, part.at[ids(k)[2], up], fy.at[k, up], yn)

    def rs_z(k):
        return link(11, k, part.at[ids(k)[0]], zr.at[k], ids(k)[0])

    def spread(k):
        if k > 0:
            ag_z(k).wait_recv()
        ag_x(k).start()
        ag_y(k).start()

    def relay(k):
        ag_x(k).wait_recv()
        ag_hx(k).start()
        ag_y(k).wait_recv()
        ag_hy(k).start()

    def feed_forward(k):
        ag_hx(k).wait_recv()
        ag_hy(k).wait_recv()
        base = flip(s - lax.rem(s, 4), 4 * k)
        x = ag[pl.ds(base, 4)].reshape(4 * half, dm)
        gate = jnp.dot(x, wg[...], preferred_element_type=jnp.float32)
        upper = jnp.dot(x, wu[...], preferred_element_type=jnp.float32)
        hidden = (gate / (1.0 + jnp.exp(-gate)) * upper).astype(jnp.bfloat16)

        def columns(t, _):
            cols = pl.ds(pl.multiple_of(t * tile, tile), tile)
            prod = jnp.dot(hidden, wd[:, cols], preferred_element_type=jnp.float32)
            part[pl.ds(base, 4), :, cols] = prod.astype(jnp.bfloat16).reshape(4, half, tile)
            return 0

        lax.fori_loop(0, dm // tile, columns, 0)
        for send in (rs_d1, rs_d2, rs_px, rs_py):
            send(k).start()

    def add_relayed(k):
        rs_d1(k).wait_recv()
        at = ids(k)[2]
        part[at, up] = (part[at, up].astype(jnp.float32) + xd[k].astype(jnp.float32)).astype(jnp.bfloat16)
        rs_qy(k).start()
        rs_d2(k).wait_recv()
        at = ids(k)[1]
        part[at, down] = (part[at, down].astype(jnp.float32) + yd[k].astype(jnp.float32)).astype(jnp.bfloat16)
        rs_qx(k).start()

    def collect(k):
        for send in (rs_px, rs_py, rs_qx, rs_qy):
            send(k).wait_recv()
        at = ids(k)[0]
        summed = part[at].astype(jnp.float32) + fx[k].astype(jnp.float32) + fy[k].astype(jnp.float32)
        if k == 0:
            stream[...] = stream[...] + summed
        else:
            part[at] = summed.astype(jnp.bfloat16)
            rs_z(k).start()

    spread(0)
    for k in range(1, levels):
        ag_z(k).start()

    def forward(m, src, k):
        return sends(slot_of(m, src), slot_of(m, src), f_s.at[m, k], w_r.at[m, src], {"tp": other})

    base_c = s // per
    for m in range(3):

        def pass_on(k, _, m=m):
            src = 2 * k + c
            mine = (src == s) & (base_c == c)

            @pl.when(mine)
            def _():
                own_copy(m, s).wait()

            @pl.when(jnp.logical_not(mine))
            def _():
                forward(m, src, k).wait_recv()

            forward(m, src, k).start()
            return 0

        lax.fori_loop(0, n // 2, pass_on, 0)

    for m in range(3):

        def arrived(k, _, m=m):
            forward(m, 2 * k + other, k).wait_recv()
            return 0

        lax.fori_loop(0, n // 2, arrived, 0)

    relay(0)
    for k in range(levels + 2):
        if k + 1 < levels:
            spread(k + 1)
        if k < levels:
            feed_forward(k)
        if 1 <= k <= levels:
            add_relayed(k - 1)
        if k >= 2:
            collect(k - 2)
        if k + 1 < levels:
            relay(k + 1)
    for k in range(1, levels):
        rs_z(k).wait_recv()
    out = stream[...]
    for k in range(1, levels):
        out = out + zr[k].astype(jnp.float32)
    out_ref[...] = out.astype(jnp.bfloat16)

    mix.wait_send()
    for k in range(levels):
        for send in (ag_x, ag_y, ag_hx, ag_hy, rs_d1, rs_d2, rs_px, rs_qx, rs_py, rs_qy):
            send(k).wait_send()
        if k > 0:
            ag_z(k).wait_send()
            rs_z(k).wait_send()

    def finish_peer(k, _):
        src = lax.rem(s + n - k, n)
        att_copy(src, src).wait_send()
        qkv_copy(src, src).wait_send()
        doc_copy(src, src).wait_send()
        return 0

    lax.fori_loop(1, n, finish_peer, 0)
    for m in range(3):

        def finish_forward(k, _, m=m):
            forward(m, 2 * k + c, k).wait_send()
            return 0

        lax.fori_loop(0, n // 2, finish_forward, 0)

        def finish_weight(k, _, m=m):
            p = per * c + lax.rem(s + k, per)

            @pl.when(jnp.logical_not((p == s) & (tc == c)))
            def _():
                w_copy(m, p, k).wait_send()

            return 0

        lax.fori_loop(0, per, finish_weight, 0)


def resharded(
    resid, queries, keys, values, doc_ids, score_offset, out_weight, norm_gain,
    gate_weight, up_weight, down_weight,
):
    n, ntp = lax.axis_size("sp"), lax.axis_size("tp")
    rows, local = queries.shape
    half, two = rows // 2, 2 * (local // n)
    dm = resid.shape[1]
    width = gate_weight.shape[1] * ntp // n
    levels = n // 4
    bf, f32 = jnp.bfloat16, jnp.float32
    vmem = pl.BlockSpec(memory_space=pltpu.VMEM)
    anyw = pl.BlockSpec(memory_space=pl.ANY)
    dma = pltpu.SemaphoreType.DMA
    per = n // ntp
    block = (half, dm)
    return pl.pallas_call(
        functools.partial(layer_kernel, n),
        out_shape=jax.ShapeDtypeStruct(block, bf),
        in_specs=[vmem] * 4 + [pl.BlockSpec(memory_space=pltpu.SMEM)] + [anyw] * 3 + [vmem] * 2 + [anyw],
        out_specs=vmem,
        scratch_shapes=[
            pltpu.VMEM((n, rows + half, two), bf),
            pltpu.VMEM((n, rows + half, two), bf),
            pltpu.VMEM((n, 8, rows), jnp.int32),
            pltpu.VMEM((n, half, two), bf),
            pltpu.VMEM((n, half, two), bf),
            pltpu.VMEM((dm, width), bf),
            pltpu.VMEM((dm, width), bf),
            pltpu.VMEM((width, dm), bf),
            pltpu.VMEM(out_weight.shape, bf),
            pltpu.VMEM((rows, local), bf),
            pltpu.VMEM((2,) + block, bf),
            pltpu.VMEM(block, bf),
            pltpu.VMEM(block, f32),
            pltpu.VMEM((n,) + block, bf),
            pltpu.VMEM((n,) + block, bf),
            pltpu.VMEM((levels, half // 2, dm), bf),
            pltpu.VMEM((levels, half // 2, dm), bf),
            pltpu.VMEM((levels,) + block, bf),
            pltpu.VMEM((levels,) + block, bf),
            pltpu.VMEM((levels,) + block, bf),
            dma((n,)), dma((n,)), dma((n,)), dma((n,)), dma((n,)), dma((n,)),
            dma((3, per)), dma((3, n)), dma((3, n // 2)), dma((3,)),
            dma, dma, dma, dma((12, levels)), dma((12, levels)),
        ],
        compiler_params=pltpu.CompilerParams(has_side_effects=True, vmem_limit_bytes=60 << 20),
    )(
        queries, keys, values, jnp.broadcast_to(doc_ids[None], (8, rows)), score_offset,
        gate_weight, up_weight, down_weight, resid, norm_gain[None], out_weight,
    )


def on_device(*args):
    queries, doc_ids, score_offset, gate_weight = args[1], args[4], args[5], args[8]
    n, ntp = lax.axis_size("sp"), lax.axis_size("tp")
    dim = queries.shape[1] // score_offset.shape[0]
    fits = (
        ntp == 2
        and n >= 4
        and n & (n - 1) == 0
        and score_offset.shape[0] == n
        and 2 * dim == 128
        and doc_ids.shape[0] == 128
        and gate_weight.shape[1] * ntp % (n * 128) == 0
        and gate_weight.shape[0] % 128 == 0
    )
    return resharded(*args) if fits else windowed(*args)


def solution(mesh):
    in_specs = (
        P(("sp", "tp"), None),
        P("sp", "tp"),
        P("sp", "tp"),
        P("sp", "tp"),
        P("sp"),
        P("tp"),
        P("tp", None),
        P(),
        P("sp", "tp"),
        P("sp", "tp"),
        P("tp", "sp"),
    )
    out_specs = P(("sp", "tp"), None)
    return jax.shard_map(
        on_device, mesh=mesh, in_specs=in_specs, out_specs=out_specs, check_vma=False
    )
```

```python
import functools

import jax
import jax.numpy as jnp
from jax import lax
from jax.experimental import pallas as pl
from jax.experimental.pallas import tpu as pltpu
from jax.sharding import PartitionSpec as P


def from_behind(shard, axis, by):
    peers = lax.axis_size(axis)
    pairs = [(i, i + by) for i in range(peers) if 0 <= i + by < peers]
    return lax.ppermute(shard, axis, pairs)


def as_sent(shard):
    return jax.tree.map(lambda a: a.astype(jnp.bfloat16) if a.dtype == jnp.float32 else a, shard)


def joined(earlier, later):
    return (
        jnp.concatenate([earlier[0], later[0]], axis=0),
        jnp.concatenate([earlier[1], later[1]], axis=0),
        jnp.concatenate([earlier[2], later[2]], axis=0),
    )


def block_update(carry, block, start, context):
    queries_h, q_pos, q_docs, offsets, scale = context
    total, carried = carry
    k_block, v_block, d_block = block
    count = k_block.shape[0]
    heads = offsets.shape[0]
    head_dim = queries_h.shape[2]

    def compute():
        key_pos = start + jnp.arange(count, dtype=jnp.int32)
        live = (
            (key_pos[None, :] >= 0)
            & (key_pos[None, :] < q_pos[:, None])
            & (d_block[None, :] == q_docs[:, None])
        )
        k_heads = k_block.reshape(count, heads, head_dim)
        v_heads = v_block.reshape(count, heads, head_dim)
        scores = (
            jnp.einsum("thd,shd->hts", queries_h, k_heads, preferred_element_type=jnp.float32)
            * scale
            + offsets[:, None, None]
        )
        log_keep = jnp.where(live[None], jax.nn.log_sigmoid(-scores), 0.0)
        tail = lax.cumsum(log_keep, axis=2, reverse=True) - log_keep + carried[:, :, None]
        weight = jnp.where(live[None], jnp.exp(jax.nn.log_sigmoid(scores) + tail), 0.0).astype(
            jnp.bfloat16
        )
        added = jnp.einsum("hts,shd->thd", weight, v_heads, preferred_element_type=jnp.float32)
        return (total + added, carried + jnp.sum(log_keep, axis=2))

    reached = (start + count > 0) & (d_block[-1] >= q_docs[0])
    return lax.cond(reached, compute, lambda: carry)


def windowed(
    resid,
    queries,
    keys,
    values,
    doc_ids,
    score_offset,
    out_weight,
    norm_gain,
    gate_weight,
    up_weight,
    down_weight,
):
    rows = queries.shape[0]
    heads = score_offset.shape[0]
    head_dim = queries.shape[1] // heads
    base = lax.axis_index("sp") * rows
    q_pos = base + jnp.arange(rows, dtype=jnp.int32)
    context = (
        queries.reshape(rows, heads, head_dim),
        q_pos,
        doc_ids,
        score_offset,
        head_dim ** (-0.5),
    )
    own = (keys, values, doc_ids)
    carry = (jnp.zeros((rows, heads, head_dim), jnp.float32), jnp.zeros((heads, rows), jnp.float32))
    nearest = from_behind((keys, values, doc_ids), "sp", 1)
    paired = joined(nearest, own)
    carry = block_update(carry, paired, base - rows, context)
    middle = from_behind((paired[0], paired[1], as_sent(paired[2])), "sp", 2)
    carry = block_update(carry, middle, base - 3 * rows, context)
    fourfold = joined(middle, paired)
    farthest = from_behind((fourfold[0], fourfold[1], as_sent(fourfold[2])), "sp", 4)
    carry = block_update(
        carry, tuple((piece[2 * rows :] for piece in farthest)), base - 5 * rows, context
    )
    carry = block_update(
        carry, tuple((piece[: 2 * rows] for piece in farthest)), base - 7 * rows, context
    )
    attended = carry[0].reshape(rows, heads * head_dim).astype(jnp.bfloat16)
    mixed_attn = lax.psum_scatter(
        jnp.dot(attended, out_weight, preferred_element_type=jnp.float32).astype(jnp.bfloat16),
        "tp",
        scatter_dimension=0,
        tiled=True,
    ).astype(jnp.float32)
    stream = resid.astype(jnp.float32) + mixed_attn
    normed = (
        stream * lax.rsqrt(jnp.mean(stream * stream, axis=1, keepdims=True) + 1e-06) * norm_gain
    ).astype(jnp.bfloat16)
    span_rows = lax.all_gather(normed, "tp", axis=0, tiled=True)
    gate = jnp.dot(
        span_rows,
        lax.all_gather(gate_weight, "sp", axis=0, tiled=True),
        preferred_element_type=jnp.float32,
    )
    upper = jnp.dot(
        span_rows,
        lax.all_gather(up_weight, "sp", axis=0, tiled=True),
        preferred_element_type=jnp.float32,
    )
    hidden = (jax.nn.silu(gate) * upper).astype(jnp.bfloat16)
    partial_out = jnp.dot(
        hidden,
        lax.all_gather(down_weight, "sp", axis=1, tiled=True),
        preferred_element_type=jnp.float32,
    )
    feed = lax.psum_scatter(
        partial_out.astype(jnp.bfloat16), "tp", scatter_dimension=0, tiled=True
    ).astype(jnp.float32)
    return (stream + feed).astype(jnp.bfloat16)


DOC_MOST = 896
MESH = pl.DeviceIdType.MESH


def sends(src, dst, send, recv, target):
    return pltpu.make_async_remote_copy(
        src_ref=src, dst_ref=dst, send_sem=send, recv_sem=recv, device_id=target, device_id_type=MESH
    )


def layer_kernel(
    n,
    q_ref, k_ref, v_ref, doc_ref, off_ref, g_in, u_in, d_in, resid_ref, gain_ref, o_in,
    out_ref,
    sbuf, rbuf, docr, ao, att_ref, wg, wu, wd, ow,
    attd, mixed, mixed_in, stream, ag, part, xd, yd, fx, fy, zr,
    qkv_s, qkv_r, doc_s, doc_r, att_s, att_r, w_s, w_r, f_s, own_sem, o_sem, mix_s, mix_r, net_s, net_r,
):
    s = lax.axis_index("sp")
    c = lax.axis_index("tp")
    rows = q_ref.shape[0]
    half = rows // 2
    dim = q_ref.shape[1] // n
    ntp = wg.shape[1] * n // g_in.shape[1]
    per = n // ntp
    width = wg.shape[1]
    depth = g_in.shape[0]
    dcols = d_in.shape[1]
    back = -(-DOC_MOST // rows)
    other = 1 - c
    barrier = pltpu.get_barrier_semaphore()

    def greet(k, _):
        pl.semaphore_signal(barrier, inc=1, device_id={"sp": lax.rem(s + k, n)}, device_id_type=MESH)
        return 0

    lax.fori_loop(1, n, greet, 0)
    pl.semaphore_signal(barrier, inc=1, device_id={"tp": other}, device_id_type=MESH)
    pltpu.make_async_copy(o_in, ow, o_sem).start()

    for j in range(n // 2):
        cols = slice(j * 2 * dim, (j + 1) * 2 * dim)
        kp, vp, qp = (r[:, cols].astype(jnp.float32) for r in (k_ref, v_ref, q_ref))
        low = lax.broadcasted_iota(jnp.int32, (rows, 2 * dim), 1) < dim
        lowh = low[:half]
        top, bot = qp[:half], qp[half:]
        sbuf[2 * j, :rows, :] = jnp.where(low, kp, pltpu.roll(vp, dim, 1)).astype(jnp.bfloat16)
        sbuf[2 * j + 1, :rows, :] = jnp.where(low, pltpu.roll(kp, dim, 1), vp).astype(jnp.bfloat16)
        sbuf[2 * j, rows:, :] = jnp.where(lowh, top, pltpu.roll(bot, dim, 1)).astype(jnp.bfloat16)
        sbuf[2 * j + 1, rows:, :] = jnp.where(lowh, pltpu.roll(top, dim, 1), bot).astype(jnp.bfloat16)

    pl.semaphore_wait(barrier, n)

    def qkv_copy(t, src):
        return sends(sbuf.at[t], rbuf.at[src], qkv_s.at[t], qkv_r.at[src], {"sp": t})

    def doc_copy(t, src):
        return sends(doc_ref, docr.at[src], doc_s.at[t], doc_r.at[src], {"sp": t})

    def start_peer(k, _):
        t = lax.rem(s + k, n)
        qkv_copy(t, s).start()
        doc_copy(t, s).start()
        return 0

    lax.fori_loop(1, n, start_peer, 0)
    rbuf[pl.ds(s, 1)] = sbuf[pl.ds(s, 1)]
    docr[pl.ds(s, 1)] = doc_ref[...][None]

    tc = c
    mats = ((g_in, wg), (u_in, wu), (d_in, wd))

    def part_of(m, p):
        start = pl.multiple_of((p - per * c) * width, width)
        return mats[m][0].at[pl.ds(start, width), :] if m == 2 else mats[m][0].at[:, pl.ds(start, width)]

    def slot_of(m, src):
        if m == 2:
            return mats[m][1].at[:, pl.ds(pl.multiple_of(src * dcols, dcols), dcols)]
        return mats[m][1].at[pl.ds(pl.multiple_of(src * depth, depth), depth), :]

    def w_copy(m, p, k):
        return sends(part_of(m, p), slot_of(m, s), w_s.at[m, k], w_r.at[m, s], {"sp": p, "tp": tc})

    def own_copy(m, p):
        return pltpu.make_async_copy(part_of(m, p), slot_of(m, s), own_sem.at[m])

    def start_weights(m):
        def start_weight(k, _):
            p = per * c + lax.rem(s + k, per)
            mine = (p == s) & (tc == c)

            @pl.when(mine)
            def _():
                own_copy(m, p).start()

            @pl.when(jnp.logical_not(mine))
            def _():
                w_copy(m, p, k).start()

            return 0

        lax.fori_loop(0, per, start_weight, 0)

    start_weights(0)
    start_weights(1)

    def wait_peer(k, _):
        src = lax.rem(s + n - k, n)
        qkv_copy(src, src).wait_recv()
        doc_copy(src, src).wait_recv()
        return 0

    lax.fori_loop(1, n, wait_peer, 0)

    scale = dim ** (-0.5)
    off = off_ref[s]
    lane = lax.broadcasted_iota(jnp.int32, (half, 2 * dim), 1) < dim
    row_i = lax.broadcasted_iota(jnp.int32, (rows, rows), 0)
    col_i = lax.broadcasted_iota(jnp.int32, (rows, rows), 1)
    later = (row_i > col_i).astype(jnp.bfloat16)
    nt = (((1,), (1,)), ((), ()))

    def att_copy(t, src):
        return sends(ao.at[t], att_ref.at[src], att_s.at[t], att_r.at[src], {"sp": t})

    def block(step, _):
        i = lax.rem(s + step, n)
        q2 = rbuf[i, rows:, :].astype(jnp.float32)
        q_pad = jnp.concatenate(
            [jnp.where(lane, q2, 0.0), jnp.where(lane, pltpu.roll(q2, dim, 1), 0.0)], axis=0
        ).astype(jnp.bfloat16)
        q_doc = jnp.broadcast_to(docr[i, 0:1, :].astype(jnp.float32), (rows, rows)).T
        total = jnp.zeros((rows, 2 * dim), jnp.float32)
        carried = jnp.zeros((rows, 1), jnp.float32)
        for d in range(min(back, n - 1) + 1):
            j = jnp.maximum(i - d, 0)
            kv = rbuf[j, :rows, :]
            k_doc = jnp.where(i >= d, docr[j, 0:1, :].astype(jnp.float32), -1.0)
            z = lax.dot_general(q_pad, kv, nt, preferred_element_type=jnp.float32) * scale + off
            live = q_doc == k_doc
            if d == 0:
                live = live & (col_i < row_i)
            soft = jnp.log(1.0 + jnp.exp(-jnp.abs(z)))
            keep = jnp.where(live, -jnp.maximum(z, 0.0) - soft, 0.0)
            high = keep.astype(jnp.bfloat16)
            rest = (keep - high.astype(jnp.float32)).astype(jnp.bfloat16)
            tail = jnp.dot(high, later, preferred_element_type=jnp.float32) + jnp.dot(
                rest, later, preferred_element_type=jnp.float32
            )
            weight = jnp.where(
                live, jnp.exp(jnp.minimum(z, 0.0) - soft + (tail + carried)), 0.0
            ).astype(jnp.bfloat16)
            total = total + jnp.dot(weight, kv, preferred_element_type=jnp.float32)
            carried = carried + jnp.sum(keep, axis=1, keepdims=True)
        packed = jnp.where(lane, pltpu.roll(total[:half], dim, 1), total[half:]).astype(jnp.bfloat16)

        @pl.when(i == s)
        def _():
            att_ref[pl.ds(s, 1)] = packed[None]

        @pl.when(i != s)
        def _():
            ao[pl.ds(i, 1)] = packed[None]
            att_copy(i, s).start()

        return 0

    lax.fori_loop(0, n, block, 0)

    start_weights(2)

    def wait_attended(k, _):
        src = lax.rem(s + n - k, n)
        att_copy(src, src).wait_recv()
        return 0

    lax.fori_loop(1, n, wait_attended, 0)
    for j in range(n // 2):
        cols = slice(j * 2 * dim, (j + 1) * 2 * dim)
        ha, hb = (att_ref[2 * j + e].astype(jnp.float32) for e in range(2))
        attd[:half, cols] = jnp.where(lane, ha, pltpu.roll(hb, dim, 1)).astype(jnp.bfloat16)
        attd[half:, cols] = jnp.where(lane, pltpu.roll(ha, dim, 1), hb).astype(jnp.bfloat16)

    pltpu.make_async_copy(o_in, ow, o_sem).wait()
    dm = ow.shape[1]
    tile = min(512, dm)

    def project(t, _):
        cols = pl.ds(pl.multiple_of(t * tile, tile), tile)
        prod = jnp.dot(attd[...], ow[:, cols], preferred_element_type=jnp.float32).astype(jnp.bfloat16)
        mixed[0, :, cols] = prod[:half]
        mixed[1, :, cols] = prod[half:]
        return 0

    lax.fori_loop(0, dm // tile, project, 0)
    mix = sends(mixed.at[other], mixed_in, mix_s, mix_r, {"tp": other})
    mix.start()
    mix.wait_recv()
    rows_f = resid_ref[...].astype(jnp.float32) + (
        mixed[c].astype(jnp.float32) + mixed_in[...].astype(jnp.float32)
    )
    stream[...] = rows_f
    inv = lax.rsqrt(jnp.mean(rows_f * rows_f, axis=1, keepdims=True) + 1e-06)
    ag[pl.ds(s, 1)] = (rows_f * inv * gain_ref[...]).astype(jnp.bfloat16)[None]

    levels = n // 4
    quarter = half // 2
    up, down = slice(0, quarter), slice(quarter, half)

    def flip(v, mask):
        bit = 1
        moved = v
        while bit <= mask:
            if mask & bit:
                moved = moved + bit - 2 * bit * lax.rem(lax.div(v, bit), 2)
            bit *= 2
        return moved

    xn, yn = flip(s, 1), flip(s, 2)

    def link(kind, k, src, dst, to):
        return sends(src, dst, net_s.at[kind, k], net_r.at[kind, k], {"sp": to})

    def ids(k):
        return tuple(flip(s, 4 * k + e) for e in range(4))

    def ag_z(k):
        return link(0, k, ag.at[s], ag.at[s], ids(k)[0])

    def ag_x(k):
        return link(1, k, ag.at[ids(k)[0]], ag.at[ids(k)[0]], xn)

    def ag_y(k):
        return link(2, k, ag.at[ids(k)[0]], ag.at[ids(k)[0]], yn)

    def ag_hx(k):
        return link(3, k, ag.at[ids(k)[1], up], ag.at[ids(k)[1], up], yn)

    def ag_hy(k):
        return link(4, k, ag.at[ids(k)[2], down], ag.at[ids(k)[2], down], xn)

    def rs_d1(k):
        return link(5, k, part.at[ids(k)[3], up], xd.at[k], xn)

    def rs_d2(k):
        return link(6, k, part.at[ids(k)[3], down], yd.at[k], yn)

    def rs_px(k):
        return link(7, k, part.at[ids(k)[1], up], fx.at[k, up], xn)

    def rs_qx(k):
        return link(8, k, part.at[ids(k)[1], down], fx.at[k, down], xn)

    def rs_py(k):
        return link(9, k, part.at[ids(k)[2], down], fy.at[k, down], yn)

    def rs_qy(k):
        return link(10, k, part.at[ids(k)[2], up], fy.at[k, up], yn)

    def rs_z(k):
        return link(11, k, part.at[ids(k)[0]], zr.at[k], ids(k)[0])

    def forward(m, src, k):
        return sends(slot_of(m, src), slot_of(m, src), f_s.at[m, k], w_r.at[m, src], {"tp": other})

    base_c = s // per
    def hand_on(m):
        def pass_on(src, _):
            mine = src == s

            @pl.when(mine)
            def _():
                own_copy(m, s).wait()

            @pl.when(jnp.logical_not(mine))
            def _():
                forward(m, src, src).wait_recv()

            forward(m, src, src).start()
            return 0

        @pl.when(base_c == c)
        def _():
            lax.fori_loop(0, n, pass_on, 0)

    def arrive(m):
        def arrived(src, _):
            forward(m, src, src).wait_recv()
            return 0

        @pl.when(base_c != c)
        def _():
            lax.fori_loop(0, n, arrived, 0)

    def spread(k):
        if k > 0:
            ag_z(k).wait_recv()
        ag_x(k).start()
        ag_y(k).start()

    def relay(k):
        ag_x(k).wait_recv()
        ag_hx(k).start()
        ag_y(k).wait_recv()
        ag_hy(k).start()

    def feed_forward(k):
        ag_hx(k).wait_recv()
        ag_hy(k).wait_recv()
        if k == order[0]:
            for m in range(2):
                hand_on(m)
            for m in range(2):
                arrive(m)
        base = flip(s - lax.rem(s, 4), 4 * k)
        x = ag[pl.ds(base, 4)].reshape(4 * half, dm)
        gate = jnp.dot(x, wg[...], preferred_element_type=jnp.float32)
        upper = jnp.dot(x, wu[...], preferred_element_type=jnp.float32)
        hidden = (gate / (1.0 + jnp.exp(-gate)) * upper).astype(jnp.bfloat16)

        if k == order[0]:
            hand_on(2)
            arrive(2)

        def columns(t, _):
            cols = pl.ds(pl.multiple_of(t * tile, tile), tile)
            prod = jnp.dot(hidden, wd[:, cols], preferred_element_type=jnp.float32)
            part[pl.ds(base, 4), :, cols] = prod.astype(jnp.bfloat16).reshape(4, half, tile)
            return 0

        lax.fori_loop(0, dm // tile, columns, 0)
        for send in (rs_d1, rs_d2, rs_px, rs_py):
            send(k).start()

    def add_relayed(k):
        rs_d1(k).wait_recv()
        at = ids(k)[2]
        part[at, up] = (part[at, up].astype(jnp.float32) + xd[k].astype(jnp.float32)).astype(jnp.bfloat16)
        rs_qy(k).start()
        rs_d2(k).wait_recv()
        at = ids(k)[1]
        part[at, down] = (part[at, down].astype(jnp.float32) + yd[k].astype(jnp.float32)).astype(jnp.bfloat16)
        rs_qx(k).start()

    def collect(k):
        for send in (rs_px, rs_py, rs_qx, rs_qy):
            send(k).wait_recv()
        at = ids(k)[0]
        summed = part[at].astype(jnp.float32) + fx[k].astype(jnp.float32) + fy[k].astype(jnp.float32)
        if k == 0:
            stream[...] = stream[...] + summed
        else:
            part[at] = summed.astype(jnp.bfloat16)
            rs_z(k).start()

    spread(0)
    for k in range(1, levels):
        ag_z(k).start()
    ahead = min(levels, 2)
    for k in range(ahead):
        if k > 0:
            spread(k)
        relay(k)
    order = [*range(1, levels), 0]
    for at in range(levels + 2):
        if at + ahead < levels:
            spread(at + ahead)
        if at < levels:
            feed_forward(order[at])
        if 1 <= at <= levels:
            add_relayed(order[at - 1])
        if at >= 2:
            collect(order[at - 2])
        if at + ahead < levels:
            relay(at + ahead)
    for k in range(1, levels):
        rs_z(k).wait_recv()
    out = stream[...]
    for k in range(1, levels):
        out = out + zr[k].astype(jnp.float32)
    out_ref[...] = out.astype(jnp.bfloat16)

    mix.wait_send()
    for k in range(levels):
        for send in (ag_x, ag_y, ag_hx, ag_hy, rs_d1, rs_d2, rs_px, rs_qx, rs_py, rs_qy):
            send(k).wait_send()
        if k > 0:
            ag_z(k).wait_send()
            rs_z(k).wait_send()

    def finish_peer(k, _):
        src = lax.rem(s + n - k, n)
        att_copy(src, src).wait_send()
        qkv_copy(src, src).wait_send()
        doc_copy(src, src).wait_send()
        return 0

    lax.fori_loop(1, n, finish_peer, 0)
    for m in range(3):

        def finish_forward(src, _, m=m):
            forward(m, src, src).wait_send()
            return 0

        @pl.when(base_c == c)
        def _():
            lax.fori_loop(0, n, finish_forward, 0)

        def finish_weight(k, _, m=m):
            p = per * c + lax.rem(s + k, per)

            @pl.when(jnp.logical_not((p == s) & (tc == c)))
            def _():
                w_copy(m, p, k).wait_send()

            return 0

        lax.fori_loop(0, per, finish_weight, 0)


def resharded(
    resid, queries, keys, values, doc_ids, score_offset, out_weight, norm_gain,
    gate_weight, up_weight, down_weight,
):
    n, ntp = lax.axis_size("sp"), lax.axis_size("tp")
    rows, local = queries.shape
    half, two = rows // 2, 2 * (local // n)
    dm = resid.shape[1]
    width = gate_weight.shape[1] * ntp // n
    levels = n // 4
    bf, f32 = jnp.bfloat16, jnp.float32
    vmem = pl.BlockSpec(memory_space=pltpu.VMEM)
    anyw = pl.BlockSpec(memory_space=pl.ANY)
    dma = pltpu.SemaphoreType.DMA
    per = n // ntp
    block = (half, dm)
    return pl.pallas_call(
        functools.partial(layer_kernel, n),
        out_shape=jax.ShapeDtypeStruct(block, bf),
        in_specs=[vmem] * 4 + [pl.BlockSpec(memory_space=pltpu.SMEM)] + [anyw] * 3 + [vmem] * 2 + [anyw],
        out_specs=vmem,
        scratch_shapes=[
            pltpu.VMEM((n, rows + half, two), bf),
            pltpu.VMEM((n, rows + half, two), bf),
            pltpu.VMEM((n, 8, rows), jnp.int32),
            pltpu.VMEM((n, half, two), bf),
            pltpu.VMEM((n, half, two), bf),
            pltpu.VMEM((dm, width), bf),
            pltpu.VMEM((dm, width), bf),
            pltpu.VMEM((width, dm), bf),
            pltpu.VMEM(out_weight.shape, bf),
            pltpu.VMEM((rows, local), bf),
            pltpu.VMEM((2,) + block, bf),
            pltpu.VMEM(block, bf),
            pltpu.VMEM(block, f32),
            pltpu.VMEM((n,) + block, bf),
            pltpu.VMEM((n,) + block, bf),
            pltpu.VMEM((levels, half // 2, dm), bf),
            pltpu.VMEM((levels, half // 2, dm), bf),
            pltpu.VMEM((levels,) + block, bf),
            pltpu.VMEM((levels,) + block, bf),
            pltpu.VMEM((levels,) + block, bf),
            dma((n,)), dma((n,)), dma((n,)), dma((n,)), dma((n,)), dma((n,)),
            dma((3, per)), dma((3, n)), dma((3, n)), dma((3,)),
            dma, dma, dma, dma((12, levels)), dma((12, levels)),
        ],
        compiler_params=pltpu.CompilerParams(has_side_effects=True, collective_id=0, vmem_limit_bytes=60 << 20),
    )(
        queries, keys, values, jnp.broadcast_to(doc_ids[None], (8, rows)), score_offset,
        gate_weight, up_weight, down_weight, resid, norm_gain[None], out_weight,
    )


def on_device(*args):
    queries, doc_ids, score_offset, gate_weight = args[1], args[4], args[5], args[8]
    n, ntp = lax.axis_size("sp"), lax.axis_size("tp")
    dim = queries.shape[1] // score_offset.shape[0]
    fits = (
        ntp == 2
        and n >= 4
        and n & (n - 1) == 0
        and score_offset.shape[0] == n
        and 2 * dim == 128
        and doc_ids.shape[0] == 128
        and gate_weight.shape[1] * ntp % (n * 128) == 0
        and gate_weight.shape[0] % 128 == 0
    )
    return resharded(*args) if fits else windowed(*args)


def solution(mesh):
    in_specs = (
        P(("sp", "tp"), None),
        P("sp", "tp"),
        P("sp", "tp"),
        P("sp", "tp"),
        P("sp"),
        P("tp"),
        P("tp", None),
        P(),
        P("sp", "tp"),
        P("sp", "tp"),
        P("tp", "sp"),
    )
    out_specs = P(("sp", "tp"), None)
    return jax.shard_map(
        on_device, mesh=mesh, in_specs=in_specs, out_specs=out_specs, check_vma=False
    )
```

```python
import functools

import jax
import jax.numpy as jnp
from jax import lax
from jax.experimental import pallas as pl
from jax.experimental.pallas import tpu as pltpu
from jax.sharding import PartitionSpec as P


def from_behind(shard, axis, by):
    peers = lax.axis_size(axis)
    pairs = [(i, i + by) for i in range(peers) if 0 <= i + by < peers]
    return lax.ppermute(shard, axis, pairs)


def as_sent(shard):
    return jax.tree.map(lambda a: a.astype(jnp.bfloat16) if a.dtype == jnp.float32 else a, shard)


def joined(earlier, later):
    return (
        jnp.concatenate([earlier[0], later[0]], axis=0),
        jnp.concatenate([earlier[1], later[1]], axis=0),
        jnp.concatenate([earlier[2], later[2]], axis=0),
    )


def block_update(carry, block, start, context):
    queries_h, q_pos, q_docs, offsets, scale = context
    total, carried = carry
    k_block, v_block, d_block = block
    count = k_block.shape[0]
    heads = offsets.shape[0]
    head_dim = queries_h.shape[2]

    def compute():
        key_pos = start + jnp.arange(count, dtype=jnp.int32)
        live = (
            (key_pos[None, :] >= 0)
            & (key_pos[None, :] < q_pos[:, None])
            & (d_block[None, :] == q_docs[:, None])
        )
        k_heads = k_block.reshape(count, heads, head_dim)
        v_heads = v_block.reshape(count, heads, head_dim)
        scores = (
            jnp.einsum("thd,shd->hts", queries_h, k_heads, preferred_element_type=jnp.float32)
            * scale
            + offsets[:, None, None]
        )
        log_keep = jnp.where(live[None], jax.nn.log_sigmoid(-scores), 0.0)
        tail = lax.cumsum(log_keep, axis=2, reverse=True) - log_keep + carried[:, :, None]
        weight = jnp.where(live[None], jnp.exp(jax.nn.log_sigmoid(scores) + tail), 0.0).astype(
            jnp.bfloat16
        )
        added = jnp.einsum("hts,shd->thd", weight, v_heads, preferred_element_type=jnp.float32)
        return (total + added, carried + jnp.sum(log_keep, axis=2))

    reached = (start + count > 0) & (d_block[-1] >= q_docs[0])
    return lax.cond(reached, compute, lambda: carry)


def windowed(
    resid,
    queries,
    keys,
    values,
    doc_ids,
    score_offset,
    out_weight,
    norm_gain,
    gate_weight,
    up_weight,
    down_weight,
):
    rows = queries.shape[0]
    heads = score_offset.shape[0]
    head_dim = queries.shape[1] // heads
    base = lax.axis_index("sp") * rows
    q_pos = base + jnp.arange(rows, dtype=jnp.int32)
    context = (
        queries.reshape(rows, heads, head_dim),
        q_pos,
        doc_ids,
        score_offset,
        head_dim ** (-0.5),
    )
    own = (keys, values, doc_ids)
    carry = (jnp.zeros((rows, heads, head_dim), jnp.float32), jnp.zeros((heads, rows), jnp.float32))
    nearest = from_behind((keys, values, doc_ids), "sp", 1)
    paired = joined(nearest, own)
    carry = block_update(carry, paired, base - rows, context)
    middle = from_behind((paired[0], paired[1], as_sent(paired[2])), "sp", 2)
    carry = block_update(carry, middle, base - 3 * rows, context)
    fourfold = joined(middle, paired)
    farthest = from_behind((fourfold[0], fourfold[1], as_sent(fourfold[2])), "sp", 4)
    carry = block_update(
        carry, tuple((piece[2 * rows :] for piece in farthest)), base - 5 * rows, context
    )
    carry = block_update(
        carry, tuple((piece[: 2 * rows] for piece in farthest)), base - 7 * rows, context
    )
    attended = carry[0].reshape(rows, heads * head_dim).astype(jnp.bfloat16)
    mixed_attn = lax.psum_scatter(
        jnp.dot(attended, out_weight, preferred_element_type=jnp.float32).astype(jnp.bfloat16),
        "tp",
        scatter_dimension=0,
        tiled=True,
    ).astype(jnp.float32)
    stream = resid.astype(jnp.float32) + mixed_attn
    normed = (
        stream * lax.rsqrt(jnp.mean(stream * stream, axis=1, keepdims=True) + 1e-06) * norm_gain
    ).astype(jnp.bfloat16)
    span_rows = lax.all_gather(normed, "tp", axis=0, tiled=True)
    gate = jnp.dot(
        span_rows,
        lax.all_gather(gate_weight, "sp", axis=0, tiled=True),
        preferred_element_type=jnp.float32,
    )
    upper = jnp.dot(
        span_rows,
        lax.all_gather(up_weight, "sp", axis=0, tiled=True),
        preferred_element_type=jnp.float32,
    )
    hidden = (jax.nn.silu(gate) * upper).astype(jnp.bfloat16)
    partial_out = jnp.dot(
        hidden,
        lax.all_gather(down_weight, "sp", axis=1, tiled=True),
        preferred_element_type=jnp.float32,
    )
    feed = lax.psum_scatter(
        partial_out.astype(jnp.bfloat16), "tp", scatter_dimension=0, tiled=True
    ).astype(jnp.float32)
    return (stream + feed).astype(jnp.bfloat16)


DOC_MOST = 896
MESH = pl.DeviceIdType.MESH


def sends(src, dst, send, recv, target):
    return pltpu.make_async_remote_copy(
        src_ref=src, dst_ref=dst, send_sem=send, recv_sem=recv, device_id=target, device_id_type=MESH
    )


def layer_kernel(
    n,
    q_ref, k_ref, v_ref, doc_ref, off_ref, g_in, u_in, d_in, resid_ref, gain_ref, o_in,
    out_ref,
    sbuf, rbuf, docr, ao, att_ref, wg, wu, wd, ow,
    attd, mixed, mixed_in, stream, ag, part, xd, yd, fx, fy, zr,
    qkv_s, qkv_r, doc_s, doc_r, att_s, att_r, w_s, w_r, f_s, own_sem, o_sem, mix_s, mix_r, net_s, net_r,
):
    s = lax.axis_index("sp")
    c = lax.axis_index("tp")
    rows = q_ref.shape[0]
    half = rows // 2
    dim = q_ref.shape[1] // n
    ntp = wg.shape[1] * n // g_in.shape[1]
    per = n // ntp
    width = wg.shape[1]
    depth = g_in.shape[0]
    dcols = d_in.shape[1]
    back = -(-DOC_MOST // rows)
    other = 1 - c
    barrier = pltpu.get_barrier_semaphore()

    def greet(k, _):
        pl.semaphore_signal(barrier, inc=1, device_id={"sp": lax.rem(s + k, n)}, device_id_type=MESH)
        return 0

    lax.fori_loop(1, n, greet, 0)
    pl.semaphore_signal(barrier, inc=1, device_id={"tp": other}, device_id_type=MESH)
    pltpu.make_async_copy(o_in, ow, o_sem).start()

    for j in range(n // 2):
        cols = slice(j * 2 * dim, (j + 1) * 2 * dim)
        kp, vp, qp = (r[:, cols].astype(jnp.float32) for r in (k_ref, v_ref, q_ref))
        low = lax.broadcasted_iota(jnp.int32, (rows, 2 * dim), 1) < dim
        lowh = low[:half]
        top, bot = qp[:half], qp[half:]
        sbuf[2 * j, :rows, :] = jnp.where(low, kp, pltpu.roll(vp, dim, 1)).astype(jnp.bfloat16)
        sbuf[2 * j + 1, :rows, :] = jnp.where(low, pltpu.roll(kp, dim, 1), vp).astype(jnp.bfloat16)
        sbuf[2 * j, rows:, :] = jnp.where(lowh, top, pltpu.roll(bot, dim, 1)).astype(jnp.bfloat16)
        sbuf[2 * j + 1, rows:, :] = jnp.where(lowh, pltpu.roll(top, dim, 1), bot).astype(jnp.bfloat16)

    pl.semaphore_wait(barrier, n)

    def qkv_copy(t, src):
        return sends(sbuf.at[t], rbuf.at[src], qkv_s.at[t], qkv_r.at[src], {"sp": t})

    def doc_copy(t, src):
        return sends(doc_ref, docr.at[src], doc_s.at[t], doc_r.at[src], {"sp": t})

    def start_peer(k, _):
        t = lax.rem(s + k, n)
        qkv_copy(t, s).start()
        doc_copy(t, s).start()
        return 0

    lax.fori_loop(1, n, start_peer, 0)
    rbuf[pl.ds(s, 1)] = sbuf[pl.ds(s, 1)]
    docr[pl.ds(s, 1)] = doc_ref[...][None]

    tc = c
    mats = ((g_in, wg), (u_in, wu), (d_in, wd))

    def part_of(m, p):
        start = pl.multiple_of((p - per * c) * width, width)
        return mats[m][0].at[pl.ds(start, width), :] if m == 2 else mats[m][0].at[:, pl.ds(start, width)]

    def slot_of(m, src):
        if m == 2:
            return mats[m][1].at[:, pl.ds(pl.multiple_of(src * dcols, dcols), dcols)]
        return mats[m][1].at[pl.ds(pl.multiple_of(src * depth, depth), depth), :]

    def w_copy(m, p, k):
        return sends(part_of(m, p), slot_of(m, s), w_s.at[m, k], w_r.at[m, s], {"sp": p, "tp": tc})

    def own_copy(m, p):
        return pltpu.make_async_copy(part_of(m, p), slot_of(m, s), own_sem.at[m])

    def start_weights(m):
        def start_weight(k, _):
            p = per * c + lax.rem(s + k, per)
            mine = (p == s) & (tc == c)

            @pl.when(mine)
            def _():
                own_copy(m, p).start()

            @pl.when(jnp.logical_not(mine))
            def _():
                w_copy(m, p, k).start()

            return 0

        lax.fori_loop(0, per, start_weight, 0)

    start_weights(0)
    start_weights(1)

    def wait_peer(k, _):
        src = lax.rem(s + n - k, n)
        qkv_copy(src, src).wait_recv()
        doc_copy(src, src).wait_recv()
        return 0

    lax.fori_loop(1, n, wait_peer, 0)

    scale = dim ** (-0.5)
    off = off_ref[s]
    lane = lax.broadcasted_iota(jnp.int32, (half, 2 * dim), 1) < dim
    row_i = lax.broadcasted_iota(jnp.int32, (rows, rows), 0)
    col_i = lax.broadcasted_iota(jnp.int32, (rows, rows), 1)
    later = (row_i > col_i).astype(jnp.bfloat16)
    nt = (((1,), (1,)), ((), ()))

    def att_copy(t, src):
        return sends(ao.at[t], att_ref.at[src], att_s.at[t], att_r.at[src], {"sp": t})

    def block(step, _):
        i = lax.rem(s + step, n)
        q2 = rbuf[i, rows:, :].astype(jnp.float32)
        q_pad = jnp.concatenate(
            [jnp.where(lane, q2, 0.0), jnp.where(lane, pltpu.roll(q2, dim, 1), 0.0)], axis=0
        ).astype(jnp.bfloat16)
        q_doc = jnp.broadcast_to(docr[i, 0:1, :].astype(jnp.float32), (rows, rows)).T
        total = jnp.zeros((rows, 2 * dim), jnp.float32)
        carried = jnp.zeros((rows, 1), jnp.float32)
        for d in range(min(back, n - 1) + 1):
            j = jnp.maximum(i - d, 0)
            kv = rbuf[j, :rows, :]
            k_doc = jnp.where(i >= d, docr[j, 0:1, :].astype(jnp.float32), -1.0)
            z = lax.dot_general(q_pad, kv, nt, preferred_element_type=jnp.float32) * scale + off
            live = q_doc == k_doc
            if d == 0:
                live = live & (col_i < row_i)
            soft = jnp.log(1.0 + jnp.exp(-jnp.abs(z)))
            keep = jnp.where(live, -jnp.maximum(z, 0.0) - soft, 0.0)
            high = keep.astype(jnp.bfloat16)
            rest = (keep - high.astype(jnp.float32)).astype(jnp.bfloat16)
            tail = jnp.dot(high, later, preferred_element_type=jnp.float32) + jnp.dot(
                rest, later, preferred_element_type=jnp.float32
            )
            weight = jnp.where(
                live, jnp.exp(jnp.minimum(z, 0.0) - soft + (tail + carried)), 0.0
            ).astype(jnp.bfloat16)
            total = total + jnp.dot(weight, kv, preferred_element_type=jnp.float32)
            carried = carried + jnp.sum(keep, axis=1, keepdims=True)
        packed = jnp.where(lane, pltpu.roll(total[:half], dim, 1), total[half:]).astype(jnp.bfloat16)

        @pl.when(i == s)
        def _():
            att_ref[pl.ds(s, 1)] = packed[None]

        @pl.when(i != s)
        def _():
            ao[pl.ds(i, 1)] = packed[None]
            att_copy(i, s).start()

        return 0

    lax.fori_loop(0, n, block, 0)


    def wait_attended(k, _):
        src = lax.rem(s + n - k, n)
        att_copy(src, src).wait_recv()
        return 0

    lax.fori_loop(1, n, wait_attended, 0)
    for j in range(n // 2):
        cols = slice(j * 2 * dim, (j + 1) * 2 * dim)
        ha, hb = (att_ref[2 * j + e].astype(jnp.float32) for e in range(2))
        attd[:half, cols] = jnp.where(lane, ha, pltpu.roll(hb, dim, 1)).astype(jnp.bfloat16)
        attd[half:, cols] = jnp.where(lane, pltpu.roll(ha, dim, 1), hb).astype(jnp.bfloat16)

    pltpu.make_async_copy(o_in, ow, o_sem).wait()
    dm = ow.shape[1]
    tile = min(512, dm)

    def project(t, _):
        cols = pl.ds(pl.multiple_of(t * tile, tile), tile)
        prod = jnp.dot(attd[...], ow[:, cols], preferred_element_type=jnp.float32).astype(jnp.bfloat16)
        mixed[0, :, cols] = prod[:half]
        mixed[1, :, cols] = prod[half:]
        return 0

    lax.fori_loop(0, dm // tile, project, 0)
    mix = sends(mixed.at[other], mixed_in, mix_s, mix_r, {"tp": other})
    mix.start()
    mix.wait_recv()
    rows_f = resid_ref[...].astype(jnp.float32) + (
        mixed[c].astype(jnp.float32) + mixed_in[...].astype(jnp.float32)
    )
    stream[...] = rows_f
    inv = lax.rsqrt(jnp.mean(rows_f * rows_f, axis=1, keepdims=True) + 1e-06)
    ag[pl.ds(s, 1)] = (rows_f * inv * gain_ref[...]).astype(jnp.bfloat16)[None]

    levels = n // 4
    quarter = half // 2
    up, down = slice(0, quarter), slice(quarter, half)

    def flip(v, mask):
        bit = 1
        moved = v
        while bit <= mask:
            if mask & bit:
                moved = moved + bit - 2 * bit * lax.rem(lax.div(v, bit), 2)
            bit *= 2
        return moved

    xn, yn = flip(s, 1), flip(s, 2)

    def link(kind, k, src, dst, to):
        return sends(src, dst, net_s.at[kind, k], net_r.at[kind, k], {"sp": to})

    def ids(k):
        return tuple(flip(s, 4 * k + e) for e in range(4))

    def ag_z(k):
        return link(0, k, ag.at[s], ag.at[s], ids(k)[0])

    def ag_x(k):
        return link(1, k, ag.at[ids(k)[0]], ag.at[ids(k)[0]], xn)

    def ag_y(k):
        return link(2, k, ag.at[ids(k)[0]], ag.at[ids(k)[0]], yn)

    def ag_hx(k):
        return link(3, k, ag.at[ids(k)[1], up], ag.at[ids(k)[1], up], yn)

    def ag_hy(k):
        return link(4, k, ag.at[ids(k)[2], down], ag.at[ids(k)[2], down], xn)

    def rs_d1(k):
        return link(5, k, part.at[ids(k)[3], up], xd.at[k], xn)

    def rs_d2(k):
        return link(6, k, part.at[ids(k)[3], down], yd.at[k], yn)

    def rs_px(k):
        return link(7, k, part.at[ids(k)[1], up], fx.at[k, up], xn)

    def rs_qx(k):
        return link(8, k, part.at[ids(k)[1], down], fx.at[k, down], xn)

    def rs_py(k):
        return link(9, k, part.at[ids(k)[2], down], fy.at[k, down], yn)

    def rs_qy(k):
        return link(10, k, part.at[ids(k)[2], up], fy.at[k, up], yn)

    def rs_z(k):
        return link(11, k, part.at[ids(k)[0]], zr.at[k], ids(k)[0])

    def forward(m, src, k):
        return sends(slot_of(m, src), slot_of(m, src), f_s.at[m, k], w_r.at[m, src], {"tp": other})

    base_c = s // per
    def hand_on(m):
        def pass_on(src, _):
            mine = src == s

            @pl.when(mine)
            def _():
                own_copy(m, s).wait()

            @pl.when(jnp.logical_not(mine))
            def _():
                forward(m, src, src).wait_recv()

            forward(m, src, src).start()
            return 0

        @pl.when(base_c == c)
        def _():
            lax.fori_loop(0, n, pass_on, 0)

    def arrive(m):
        def arrived(src, _):
            forward(m, src, src).wait_recv()
            return 0

        @pl.when(base_c != c)
        def _():
            lax.fori_loop(0, n, arrived, 0)

    def spread(k):
        if k > 0:
            ag_z(k).wait_recv()
        ag_x(k).start()
        ag_y(k).start()

    def relay(k):
        ag_x(k).wait_recv()
        ag_hx(k).start()
        ag_y(k).wait_recv()
        ag_hy(k).start()

    def feed_forward(k):
        ag_hx(k).wait_recv()
        ag_hy(k).wait_recv()
        if k == order[0]:
            for m in range(2):
                hand_on(m)
            for m in range(2):
                arrive(m)
        base = flip(s - lax.rem(s, 4), 4 * k)
        x = ag[pl.ds(base, 4)].reshape(4 * half, dm)
        gate = jnp.dot(x, wg[...], preferred_element_type=jnp.float32)
        upper = jnp.dot(x, wu[...], preferred_element_type=jnp.float32)
        hidden = (gate / (1.0 + jnp.exp(-gate)) * upper).astype(jnp.bfloat16)

        if k == order[0]:
            hand_on(2)
            arrive(2)

        def columns(t, _):
            cols = pl.ds(pl.multiple_of(t * tile, tile), tile)
            prod = jnp.dot(hidden, wd[:, cols], preferred_element_type=jnp.float32)
            part[pl.ds(base, 4), :, cols] = prod.astype(jnp.bfloat16).reshape(4, half, tile)
            return 0

        lax.fori_loop(0, dm // tile, columns, 0)
        for send in (rs_d1, rs_d2, rs_px, rs_py):
            send(k).start()

    def add_relayed(k):
        rs_d1(k).wait_recv()
        at = ids(k)[2]
        part[at, up] = (part[at, up].astype(jnp.float32) + xd[k].astype(jnp.float32)).astype(jnp.bfloat16)
        rs_qy(k).start()
        rs_d2(k).wait_recv()
        at = ids(k)[1]
        part[at, down] = (part[at, down].astype(jnp.float32) + yd[k].astype(jnp.float32)).astype(jnp.bfloat16)
        rs_qx(k).start()

    def collect(k):
        for send in (rs_px, rs_py, rs_qx, rs_qy):
            send(k).wait_recv()
        at = ids(k)[0]
        summed = part[at].astype(jnp.float32) + fx[k].astype(jnp.float32) + fy[k].astype(jnp.float32)
        if k == 0:
            stream[...] = stream[...] + summed
        else:
            part[at] = summed.astype(jnp.bfloat16)
            rs_z(k).start()

    spread(0)
    for k in range(1, levels):
        ag_z(k).start()
    start_weights(2)
    ahead = min(levels, 3)
    for k in range(ahead):
        if k > 0:
            spread(k)
        relay(k)
    order = [*range(1, levels), 0]
    for at in range(levels + 2):
        if at + ahead < levels:
            spread(at + ahead)
        if at < levels:
            feed_forward(order[at])
        if 1 <= at <= levels:
            add_relayed(order[at - 1])
        if at >= 2:
            collect(order[at - 2])
        if at + ahead < levels:
            relay(at + ahead)
    for k in range(1, levels):
        rs_z(k).wait_recv()
    out = stream[...]
    for k in range(1, levels):
        out = out + zr[k].astype(jnp.float32)
    out_ref[...] = out.astype(jnp.bfloat16)

    mix.wait_send()
    for k in range(levels):
        for send in (ag_x, ag_y, ag_hx, ag_hy, rs_d1, rs_d2, rs_px, rs_qx, rs_py, rs_qy):
            send(k).wait_send()
        if k > 0:
            ag_z(k).wait_send()
            rs_z(k).wait_send()

    def finish_peer(k, _):
        src = lax.rem(s + n - k, n)
        att_copy(src, src).wait_send()
        qkv_copy(src, src).wait_send()
        doc_copy(src, src).wait_send()
        return 0

    lax.fori_loop(1, n, finish_peer, 0)
    for m in range(3):

        def finish_forward(src, _, m=m):
            forward(m, src, src).wait_send()
            return 0

        @pl.when(base_c == c)
        def _():
            lax.fori_loop(0, n, finish_forward, 0)

        def finish_weight(k, _, m=m):
            p = per * c + lax.rem(s + k, per)

            @pl.when(jnp.logical_not((p == s) & (tc == c)))
            def _():
                w_copy(m, p, k).wait_send()

            return 0

        lax.fori_loop(0, per, finish_weight, 0)


def resharded(
    resid, queries, keys, values, doc_ids, score_offset, out_weight, norm_gain,
    gate_weight, up_weight, down_weight,
):
    n, ntp = lax.axis_size("sp"), lax.axis_size("tp")
    rows, local = queries.shape
    half, two = rows // 2, 2 * (local // n)
    dm = resid.shape[1]
    width = gate_weight.shape[1] * ntp // n
    levels = n // 4
    bf, f32 = jnp.bfloat16, jnp.float32
    vmem = pl.BlockSpec(memory_space=pltpu.VMEM)
    anyw = pl.BlockSpec(memory_space=pl.ANY)
    dma = pltpu.SemaphoreType.DMA
    per = n // ntp
    block = (half, dm)
    return pl.pallas_call(
        functools.partial(layer_kernel, n),
        out_shape=jax.ShapeDtypeStruct(block, bf),
        in_specs=[vmem] * 4 + [pl.BlockSpec(memory_space=pltpu.SMEM)] + [anyw] * 3 + [vmem] * 2 + [anyw],
        out_specs=vmem,
        scratch_shapes=[
            pltpu.VMEM((n, rows + half, two), bf),
            pltpu.VMEM((n, rows + half, two), bf),
            pltpu.VMEM((n, 8, rows), jnp.int32),
            pltpu.VMEM((n, half, two), bf),
            pltpu.VMEM((n, half, two), bf),
            pltpu.VMEM((dm, width), bf),
            pltpu.VMEM((dm, width), bf),
            pltpu.VMEM((width, dm), bf),
            pltpu.VMEM(out_weight.shape, bf),
            pltpu.VMEM((rows, local), bf),
            pltpu.VMEM((2,) + block, bf),
            pltpu.VMEM(block, bf),
            pltpu.VMEM(block, f32),
            pltpu.VMEM((n,) + block, bf),
            pltpu.VMEM((n,) + block, bf),
            pltpu.VMEM((levels, half // 2, dm), bf),
            pltpu.VMEM((levels, half // 2, dm), bf),
            pltpu.VMEM((levels,) + block, bf),
            pltpu.VMEM((levels,) + block, bf),
            pltpu.VMEM((levels,) + block, bf),
            dma((n,)), dma((n,)), dma((n,)), dma((n,)), dma((n,)), dma((n,)),
            dma((3, per)), dma((3, n)), dma((3, n)), dma((3,)),
            dma, dma, dma, dma((12, levels)), dma((12, levels)),
        ],
        compiler_params=pltpu.CompilerParams(has_side_effects=True, collective_id=0, vmem_limit_bytes=60 << 20),
    )(
        queries, keys, values, jnp.broadcast_to(doc_ids[None], (8, rows)), score_offset,
        gate_weight, up_weight, down_weight, resid, norm_gain[None], out_weight,
    )


def on_device(*args):
    queries, doc_ids, score_offset, gate_weight = args[1], args[4], args[5], args[8]
    n, ntp = lax.axis_size("sp"), lax.axis_size("tp")
    dim = queries.shape[1] // score_offset.shape[0]
    fits = (
        ntp == 2
        and n >= 4
        and n & (n - 1) == 0
        and score_offset.shape[0] == n
        and 2 * dim == 128
        and doc_ids.shape[0] == 128
        and gate_weight.shape[1] * ntp % (n * 128) == 0
        and gate_weight.shape[0] % 128 == 0
    )
    return resharded(*args) if fits else windowed(*args)


def solution(mesh):
    in_specs = (
        P(("sp", "tp"), None),
        P("sp", "tp"),
        P("sp", "tp"),
        P("sp", "tp"),
        P("sp"),
        P("tp"),
        P("tp", None),
        P(),
        P("sp", "tp"),
        P("sp", "tp"),
        P("tp", "sp"),
    )
    out_specs = P(("sp", "tp"), None)
    return jax.shard_map(
        on_device, mesh=mesh, in_specs=in_specs, out_specs=out_specs, check_vma=False
    )
```
